256 devices in a mesh: grp: 2 (over z), ep: 64 (over y, x), tp: 2 (over core).
Axes of the slice: x: 8, y: 8, z: 2, core: 2. Of those that a mesh axis runs over, the one named last changes fastest.
The devices are a block of a 8x8x16 slice.
Arguments:
- tokens_in: bfloat16 [8192, 2048], P(('grp', 'ep')), parts along dimension 0, may hold values from -6 to 6
- norm_gain: float32 [2048], replicated, may hold values from 0.1 to 1.9
- gate_proj: bfloat16 [64, 2048, 1024], P('ep', None, 'tp'), may hold values from -0.125 to 0.125
- up_proj: bfloat16 [64, 2048, 1024], P('ep', None, 'tp'), may hold values from -0.125 to 0.125
- down_proj: bfloat16 [64, 1024, 2048], P('ep', 'tp'), may hold values from -0.1875 to 0.1875
- route_ids: int32 [8192, 8], P(('grp', 'ep')), parts along dimension 0, may hold values from 0 to 63, all different within a row; in each aligned block of 64 rows (0 to 63, 64 to 127, ...) at most 16 rows name the same one
- group_weight: float32 [8192, 8], P(('grp', 'ep')), parts along dimension 0, may hold values from 0.05 to 1
- expert_weight: float32 [8192, 8], P(('grp', 'ep')), parts along dimension 0, may hold values from 0.05 to 1
Outputs:
- expert_mix: bfloat16 [8192, 2048], P(('grp', 'ep'), 'tp'), parts along dimension 0
The draws below stay inside these ranges and needn't reach their ends.
There are 2 independent parts, one for each index of `grp`. The reference program is written for one: setup_inputs(seed, part) draws one part's arguments, and reference() takes and returns one part's arrays. A program takes and returns all parts, laid end to end along the dimension named above; an argument that names none is the same for every part. Nothing has to cross between parts.
Inputs may be any that keep to these rules, and one draw needn't show every extreme that they name: `route_ids`: each row names 8 different experts; within the rows of one index of ep no expert is named by more than 16 rows, a bound that some of them reach.
All inputs are finite; a program needn't handle non-finite values.
Results may differ from the reference program's by a relative error of at most 0.0077.
Values may be sent and summed in bfloat16 or wider, within the bound.
A program may use at most 64 MiB of HBM per device.

```python
import math
import jax
import jax.numpy as jnp
import numpy as np
from jax import lax

D = 2048
DE = 1024
TOP = 8
EXP_GRP = 8
TOK_DEV = 64
EXPERTS = 64
GROUPS = 8
CAP = 16
TOKENS = 4096
N_EP = 64
N_TP = 2


def steps_of(own_key, dims, shards, smallest, largest):
    loudness = 1.0
    for axis_at, shards_of in shards:
        draws = jax.random.uniform(jax.random.fold_in(jax.random.fold_in(own_key, 6), axis_at), (shards_of,), jnp.float32, smallest / len(shards), largest / len(shards))
        loudness = loudness * jnp.repeat(jnp.exp(draws), dims[axis_at] // shards_of).reshape((-1,) + (1,) * (len(dims) - 1 - axis_at))
    return loudness


def shared_out(key, own, number, rows, count, top, most, skew):
    ranking = jax.random.permutation(key, count)
    crowded, usual = load_shares(count, rows * top, most, skew, True), load_shares(count, rows * top, most, skew, False)
    places = jnp.arange(count)

    def named(sizes, offset_by):
        used = int((sizes > 0).sum())
        fixed = max(1, used // 4)
        passed = fixed + (places - fixed + offset_by * (used - fixed)) % max(1, count - fixed)
        return jnp.zeros((count,), jnp.int32).at[ranking[jnp.where(places < fixed, places, passed)]].set(jnp.asarray(sizes, jnp.int32))

    sizes = jnp.where(number % 4 == 0, named(crowded, number // 4), named(usual, number - number // 4 - 1))
    mixed = jax.random.permutation(jax.random.fold_in(own, 3), count)
    giver, receiver = mixed[0:count // 2 * 2:2], mixed[1:count // 2 * 2:2]
    margin = jnp.minimum(sizes[giver] - 1, most - sizes[receiver]) // 2
    margin = jnp.where((giver == ranking[0]) | (receiver == ranking[0]) | (sizes[receiver] == 0), 0, jnp.maximum(margin, 0))
    passed = jax.random.randint(jax.random.fold_in(own, 4), (count // 2,), 0, 1 << 20) % (margin + 1)
    sizes = sizes.at[giver].add(-passed).at[receiver].add(passed)
    labels = jnp.searchsorted(jnp.cumsum(sizes), jnp.arange(rows * top), side="right").astype(jnp.int32)
    grid = labels.reshape(top, rows).T
    grid = grid[jax.random.permutation(jax.random.fold_in(own, 1), rows)]
    offset_by = jax.random.randint(jax.random.fold_in(own, 2), (rows, 1), 0, top)
    return jnp.take_along_axis(grid, (jnp.arange(top)[None, :] + offset_by) % top, axis=1)


def load_shares(number_of, total, limit, skew, full):
    portions = [(1 << 20) // math.isqrt(standing ** skew) + 1 for standing in range(1, number_of + 1)]
    largest = limit if full else min(limit, max(-(-total // number_of), total * portions[0] // sum(portions)))
    least = 1 if total - largest >= number_of - 1 else 0
    given, spare = [largest] + [least] * (number_of - 1), total - largest - least * (number_of - 1)
    while spare > 0:
        free = [i for i in range(1, number_of) if given[i] < largest] or [i for i in range(1, number_of) if given[i] < limit]
        mass, left = sum([portions[i] for i in free]), spare
        for i in free:
            addition = min(limit - given[i], max(1, left * portions[i] // mass), spare)
            given[i] = given[i] + addition
            spare = spare - addition
    return np.array(given)


def noise(stream_key, dims, deviation, limit, split=(), kind=jnp.bfloat16):
    drawn = jax.random.normal(stream_key, dims, jnp.float32) * deviation
    if len(split) > 0:
        drawn = steps_of(stream_key, dims, split, -0.22, 0.18) * drawn
    return jnp.clip(drawn, min=-limit, max=limit).astype(kind)


def setup_inputs(seed: int = 0, part: int = 0) -> dict:
    arg_keys = jax.random.split(jax.random.key(seed), 9)
    own_keys = jax.random.split(jax.random.fold_in(arg_keys[8], part), 9)
    tokens_in = noise(own_keys[0], (TOKENS, D), 1.0, 6.0, ((0, 64),))
    norm_gain = jnp.clip(1.0 + 0.18 * jax.random.normal(arg_keys[1], (D,), jnp.float32), 0.1, 1.9)
    gate_proj = noise(arg_keys[2], (EXPERTS, D, DE), D ** -0.5, 0.125, ((0, 64), (2, 2)))
    up_proj = noise(arg_keys[3], (EXPERTS, D, DE), D ** -0.5, 0.125, ((0, 64), (2, 2)))
    down_proj = noise(arg_keys[4], (EXPERTS, DE, D), DE ** -0.5, 0.1875, ((0, 64), (1, 2)))
    route_ids_keys = jax.random.split(jax.random.fold_in(own_keys[5], 1), TOKENS // TOK_DEV)
    route_ids_turns = jax.random.permutation(jax.random.fold_in(own_keys[5], 3), TOKENS // TOK_DEV)
    route_ids = jax.vmap(lambda own, number: shared_out(jax.random.fold_in(own_keys[5], 2), own, number, TOK_DEV, EXPERTS, TOP, CAP, 2))(route_ids_keys, route_ids_turns).reshape((TOKENS, TOP))
    group_weight = jnp.clip(jnp.exp(math.log(1.0) - 2.9957323 * jax.random.uniform(own_keys[6], (TOKENS, GROUPS), jnp.float32) ** steps_of(own_keys[6], (TOKENS, GROUPS), ((0, 64),), -0.2, 0.2)), 0.05, 1.0)
    expert_weight = jnp.clip(jnp.exp(math.log(1.0) - 2.9957323 * jax.random.uniform(own_keys[7], (TOKENS, TOP), jnp.float32) ** steps_of(own_keys[7], (TOKENS, TOP), ((0, 64),), -0.2, 0.2)), 0.05, 1.0)
    return dict(tokens_in=tokens_in, norm_gain=norm_gain, gate_proj=gate_proj, up_proj=up_proj, down_proj=down_proj, route_ids=route_ids, group_weight=group_weight, expert_weight=expert_weight)


EPSILON = 1e-06

def reference(tokens_in, norm_gain, gate_proj, up_proj, down_proj, route_ids, group_weight, expert_weight):
    row_values = tokens_in.astype(jnp.float32)
    inv_scale = lax.rsqrt(lax.optimization_barrier(jnp.mean(row_values * row_values, axis=-1, keepdims=True)) + EPSILON)
    normed = (row_values * inv_scale * norm_gain.astype(jnp.float32)).astype(jnp.bfloat16)
    token_count = tokens_in.shape[0]
    expert_count = gate_proj.shape[0]
    route_count = token_count * TOP
    flat_ids = route_ids.reshape(route_count).astype(jnp.int32)
    sort_order = jnp.argsort(flat_ids, stable=True).astype(jnp.int32)
    expert_counts = lax.optimization_barrier(jnp.sum((flat_ids[None, :] == jnp.arange(expert_count, dtype=jnp.int32)[:, None]).astype(jnp.int32), axis=1)).astype(jnp.int32)
    expert_starts = (jnp.cumsum(expert_counts) - expert_counts).astype(jnp.int32)
    buffer_rows = N_EP * CAP
    padded_order = jnp.concatenate([sort_order, jnp.zeros((buffer_rows,), jnp.int32)])
    half_width = DE // N_TP

    def one_expert(expert_index):
        begin_at = expert_starts[expert_index].astype(jnp.int32)
        picked = lax.dynamic_slice_in_dim(padded_order, begin_at, buffer_rows)
        is_valid = jnp.arange(buffer_rows, dtype=jnp.int32) < expert_counts[expert_index]
        source_rows = normed[picked // TOP]
        gate_acts = jnp.dot(source_rows, gate_proj[expert_index], preferred_element_type=jnp.float32)
        up_acts = jnp.dot(source_rows, up_proj[expert_index], preferred_element_type=jnp.float32)
        hidden = (jax.nn.silu(gate_acts) * up_acts).astype(jnp.bfloat16)
        total_sum = jnp.zeros((buffer_rows, D), jnp.float32)
        for lane_block in range(N_TP):
            part_sum = jnp.dot(hidden[:, lane_block * half_width:(lane_block + 1) * half_width], down_proj[expert_index, lane_block * half_width:(lane_block + 1) * half_width], preferred_element_type=jnp.float32)
            part_sum = lax.optimization_barrier(part_sum.astype(jnp.bfloat16))
            total_sum = total_sum + part_sum.astype(jnp.float32)
        target_rows = jnp.where(is_valid, picked, route_count).astype(jnp.int32)
        return (total_sum.astype(jnp.bfloat16), target_rows)
    outputs, targets = lax.map(one_expert, jnp.arange(expert_count, dtype=jnp.int32))
    per_route = jnp.zeros((route_count + 1, D), jnp.bfloat16).at[targets.reshape(-1)].set(outputs.reshape(-1, D))[:route_count]
    chosen = per_route.reshape(token_count, TOP, D).astype(jnp.float32)
    group_ids = (route_ids // EXP_GRP).astype(jnp.int32)
    group_part = jnp.take_along_axis(group_weight, group_ids, axis=1)
    gate_values = group_part * expert_weight / lax.optimization_barrier(jnp.sum(expert_weight, axis=1, keepdims=True))
    return lax.optimization_barrier(jnp.sum(chosen * gate_values[:, :, None], axis=1)).astype(jnp.bfloat16)
```

```python
import functools
import math

import jax
import jax.numpy as jnp
from jax import lax
from jax.experimental import pallas as pl
from jax.experimental.pallas import tpu as pltpu
from jax.sharding import PartitionSpec as P

TOP = 8
EXP_GRP = 8
EPSILON = 1e-06
MESH = pl.DeviceIdType.MESH
SIDE = 8
BF = jnp.bfloat16
F32 = jnp.float32

OFF = [0, 1, 7, 2, 6, 3, 5, 4]
BACK = [OFF.index((-o) % SIDE) for o in OFF]
INWARD = [7, 5, 6, 3, 4, 1, 2, 0]


def ring_offset(place):
    half = (place + 1) // 2
    odd = place % 2
    return (odd * half + (1 - odd) * (SIDE - half)) % SIDE


def moe_kernel(
    routes_ref, tokens_hbm, gain_ref, gate_hbm, up_hbm, down_hbm, out_ref,
    tok_in, toks, meta_out, meta, sel, xin, xoth, wg, wu, wd, accg, accu, hid,
    part_out, part_own, part_in, res, ret, sums_out, sums_in,
    load_sem, ag_send, ag_recv, meta_send, meta_recv, sel_send, xin_recv, xo_send, xo_recv,
    part_send, part_recv, res_send, ret_recv, sum_send, sum_recv,
):
    rows, width = tok_in.shape
    part = width // 2
    cap = sel.shape[2]
    hidden = wg.shape[2]
    grp = lax.axis_index("grp")
    ep = lax.axis_index("ep")
    core = lax.axis_index("tp")
    up_y = ep // SIDE
    up_x = ep % SIDE
    first = up_x * (1 - core) + up_y * core
    second = up_y * (1 - core) + up_x * core
    step_first = (1 - core) + SIDE * core
    step_second = SIDE * (1 - core) + core

    def along_first(place):
        at = (first + OFF[place]) % SIDE
        return (grp, at * step_first + second * step_second, core)

    def along_second(place):
        at = (second + OFF[place]) % SIDE
        return (grp, first * step_first + at * step_second, core)

    partner = (grp, ep, 1 - core)

    barrier = pltpu.get_barrier_semaphore()
    for place in range(1, SIDE):
        pl.semaphore_signal(barrier, inc=1, device_id=along_first(place), device_id_type=MESH)
        pl.semaphore_signal(barrier, inc=1, device_id=along_second(place), device_id_type=MESH)
    pl.semaphore_signal(barrier, inc=1, device_id=partner, device_id_type=MESH)

    def send(src, dst, send_sem, recv_sem, to):
        copy = pltpu.make_async_remote_copy(
            src_ref=src, dst_ref=dst, send_sem=send_sem, recv_sem=recv_sem,
            device_id=to, device_id_type=MESH,
        )
        copy.start()

    def wait_bytes(ref, sem):
        pltpu.make_async_copy(ref, ref, sem).wait()

    own = pl.ds(pl.multiple_of(core * part, part), part)
    other = pl.ds(pl.multiple_of((1 - core) * part, part), part)
    tok_load = pltpu.make_async_copy(tokens_hbm, tok_in, load_sem.at[0])
    tok_load.start()
    loads = [
        pltpu.make_async_copy(gate_hbm.at[0, own], wg.at[0], load_sem.at[1]),
        pltpu.make_async_copy(up_hbm.at[0, own], wu.at[0], load_sem.at[2]),
        pltpu.make_async_copy(gate_hbm.at[0, other], wg.at[1], load_sem.at[3]),
        pltpu.make_async_copy(up_hbm.at[0, other], wu.at[1], load_sem.at[4]),
        pltpu.make_async_copy(down_hbm.at[0, :, own], wd.at[0], load_sem.at[5]),
        pltpu.make_async_copy(down_hbm.at[0, :, other], wd.at[1], load_sem.at[6]),
    ]
    for load in loads:
        load.start()

    lanes = 2 * rows
    experts = SIDE * SIDE
    row = lax.broadcasted_iota(jnp.int32, (experts, lanes), 0)
    lane = lax.broadcasted_iota(jnp.int32, (experts, lanes), 1)
    at_first = (first + ring_offset(row // SIDE)) % SIDE
    at_second = (second + ring_offset(row % SIDE)) % SIDE
    expert = at_first * step_first + at_second * step_second
    weight_sum = jnp.sum(routes_ref[2 * TOP : 3 * TOP, :], axis=0, keepdims=True)
    named = jnp.zeros((experts, lanes), F32)
    weight = jnp.zeros((experts, lanes), F32)
    expert_f = expert.astype(F32)
    for k in range(TOP):
        match = expert_f == routes_ref[k : k + 1, :]
        named = jnp.where(match, 1.0, named)
        weight = jnp.where(match, routes_ref[2 * TOP + k : 2 * TOP + k + 1, :], weight)
    group = expert // EXP_GRP
    group_part = jnp.zeros((experts, lanes), F32)
    for g in range(experts // EXP_GRP):
        group_part = jnp.where(group == g, routes_ref[TOP + g : TOP + g + 1, :], group_part)
    gates = group_part * weight / weight_sum
    high = gates.astype(BF).astype(F32)
    gates = jnp.where(lane < rows, high, gates - high)
    before = lax.broadcasted_iota(jnp.int32, (lanes, lanes), 0)
    after = lax.broadcasted_iota(jnp.int32, (lanes, lanes), 1)
    earlier = jnp.where((before < after) & (before // rows == after // rows), 1.0, 0.0).astype(BF)
    rank = jnp.dot(named.astype(BF), earlier, preferred_element_type=F32)
    slots = jnp.where(named > 0.0, rank, -1.0)
    meta_out[:, 0] = slots.reshape(SIDE, SIDE, lanes)
    meta_out[:, 1] = gates.reshape(SIDE, SIDE, lanes)
    meta[0] = meta_out[0]

    tok_load.wait()
    values = tok_in[...].astype(F32)
    scale = lax.rsqrt(jnp.mean(values * values, axis=-1, keepdims=True) + EPSILON)
    toks[0] = (tok_in[:, own].astype(F32) * scale * gain_ref[:, own]).astype(BF)

    accg[...] = jnp.zeros_like(accg)
    accu[...] = jnp.zeros_like(accu)

    pl.semaphore_wait(barrier, 2 * (SIDE - 1) + 1)

    def pass_on(place, to_place):
        toward = BACK[1] if OFF[to_place] < SIDE // 2 else BACK[2]
        send(toks.at[place], toks.at[to_place], ag_send.at[to_place], ag_recv.at[to_place], along_first(toward))

    pass_on(0, 1)
    pass_on(0, 2)
    for place in range(1, SIDE):
        send(meta_out.at[place], meta.at[BACK[place]], meta_send.at[place], meta_recv.at[BACK[place]], along_first(place))

    slot_iota = (lax.broadcasted_iota(jnp.int32, (SIDE * cap, lanes), 0) % cap).astype(F32)

    def spread(table):
        return jnp.concatenate(
            [jnp.broadcast_to(table[j : j + 1, :], (cap, lanes)) for j in range(SIDE)], axis=0
        )

    def pick_and_send(s):
        if s > 0:
            wait_bytes(toks.at[s], ag_recv.at[s])
            if s % 2 == 1 and s < 5:
                pass_on(s, s + 2)
            elif s in (2, 4):
                pass_on(s, s + 2)
            elif s == 6:
                pass_on(s, 7)
            wait_bytes(meta.at[s], meta_recv.at[s])
        chosen = jnp.where(spread(meta[s, 0]) == slot_iota, 1.0, 0.0).astype(BF)[:, :rows]
        picked = jnp.dot(chosen, toks[s], preferred_element_type=F32).astype(BF)
        picked = picked.reshape(SIDE, cap, part)
        sel[s] = picked
        xin[s, 0] = picked[0]
        for place in range(SIDE - 1, 0, -1):
            send(sel.at[s, place], xin.at[s, BACK[place]], sel_send.at[s], xin_recv.at[s], along_second(place))

    def take_own(s):
        wait_bytes(xin.at[s, pl.ds(1, SIDE - 1)], xin_recv.at[s])
        send(xin.at[s], xoth.at[:, s], xo_send.at[s], xo_recv.at[s], partner)
        block = xin[s].reshape(SIDE * cap, part)
        accg[s] += jnp.dot(block, wg[0], preferred_element_type=F32).reshape(SIDE, cap, hidden)
        accu[s] += jnp.dot(block, wu[0], preferred_element_type=F32).reshape(SIDE, cap, hidden)

    def take_other(s):
        wait_bytes(xoth.at[:, s], xo_recv.at[s])
        block = xoth[:, s].reshape(SIDE * cap, part)
        accg[:, s] += jnp.dot(block, wg[1], preferred_element_type=F32).reshape(SIDE, cap, hidden)
        accu[:, s] += jnp.dot(block, wu[1], preferred_element_type=F32).reshape(SIDE, cap, hidden)

    for step in range(SIDE + 3):
        if step == 2:
            for load in loads:
                load.wait()
        if step < SIDE:
            pick_and_send(step)
        if 2 <= step < SIDE + 2:
            take_own(step - 2)
        if 3 <= step:
            take_other(step - 3)

    for s in range(SIDE):
        gate_acts = accg[s]
        hid[s] = (gate_acts / (1.0 + jnp.exp(-gate_acts)) * accu[s]).astype(BF)

    def multiply_down(s):
        theirs = hid[:, s].reshape(SIDE * cap, hidden)
        part_out[s] = jnp.dot(theirs, wd[1], preferred_element_type=F32).astype(BF).reshape(SIDE, cap, part)
        send(part_out.at[s], part_in.at[s], part_send.at[s], part_recv.at[s], partner)
        mine = hid[s].reshape(SIDE * cap, hidden)
        part_own[s] = jnp.dot(mine, wd[0], preferred_element_type=F32).astype(BF).reshape(SIDE, cap, part)

    def return_rows(s):
        wait_bytes(part_in.at[s], part_recv.at[s])
        res[s] = (part_own[s].astype(F32) + part_in[s].astype(F32)).astype(BF)
        ret[s, 0] = res[s, 0]
        for place in range(SIDE - 1, 0, -1):
            send(res.at[s, place], ret.at[s, BACK[place]], res_send.at[s], ret_recv.at[s], along_second(place))

    def mix(s):
        wait_bytes(ret.at[s, pl.ds(1, SIDE - 1)], ret_recv.at[s])
        mixer = jnp.where(spread(meta[s, 0]) == slot_iota, spread(meta[s, 1]), 0.0).astype(BF)
        both = lax.dot_general(
            mixer, ret[s].reshape(SIDE * cap, part), (((0,), (0,)), ((), ())), preferred_element_type=F32
        )
        total = both[:rows] + both[rows:]
        arriving = [s] if s in (1, 2, 3, 4, 5) else ([0, 6] if s == 0 else [])
        for slot in arriving:
            wait_bytes(sums_in.at[slot], sum_recv.at[slot])
            total = total + sums_in[slot].astype(F32)
        if s == 0:
            out_ref[...] = total.astype(BF)
            return
        sums_out[s] = total.astype(BF)
        to_slot = {7: 5, 5: 3, 3: 1, 1: 0, 6: 4, 4: 2, 2: 6}[s]
        toward = 1 if s % 2 == 1 else 2
        send(sums_out.at[s], sums_in.at[to_slot], sum_send.at[s], sum_recv.at[to_slot], along_first(toward))

    for step in range(SIDE + 3):
        if step < SIDE:
            multiply_down(INWARD[step])
        if 1 <= step < SIDE + 1:
            return_rows(INWARD[step - 1])
        if 3 <= step:
            mix(INWARD[step - 3])

    for place in range(1, SIDE):
        wait_bytes(toks.at[place], ag_send.at[place])
        wait_bytes(meta_out.at[place], meta_send.at[place])
        wait_bytes(sums_out.at[place], sum_send.at[place])
    for s in range(SIDE):
        wait_bytes(sel.at[s, pl.ds(1, SIDE - 1)], sel_send.at[s])
        wait_bytes(xin.at[s], xo_send.at[s])
        wait_bytes(part_out.at[s], part_send.at[s])
        wait_bytes(res.at[s, pl.ds(1, SIDE - 1)], res_send.at[s])


def on_device(
    tokens_in, norm_gain, gate_proj, up_proj, down_proj, route_ids, group_weight, expert_weight
):
    rows, width = tokens_in.shape
    experts = gate_proj.shape[0] * lax.axis_size("ep")
    hidden = gate_proj.shape[2]
    cap = min(rows, max(2, 2 * rows * TOP // experts))
    part = width // 2
    routes = jnp.concatenate(
        [route_ids.astype(F32), group_weight, expert_weight], axis=1
    ).T
    routes = jnp.concatenate([routes, routes], axis=1)
    vmem = lambda *shape: pltpu.VMEM(shape, BF)
    dma = pltpu.SemaphoreType.DMA
    blocks = (SIDE, SIDE, cap, part)
    return pl.pallas_call(
        moe_kernel,
        out_shape=jax.ShapeDtypeStruct((rows, part), BF),
        in_specs=[
            pl.BlockSpec(memory_space=pltpu.VMEM),
            pl.BlockSpec(memory_space=pl.ANY),
            pl.BlockSpec(memory_space=pltpu.VMEM),
            pl.BlockSpec(memory_space=pl.ANY),
            pl.BlockSpec(memory_space=pl.ANY),
            pl.BlockSpec(memory_space=pl.ANY),
        ],
        out_specs=pl.BlockSpec(memory_space=pltpu.VMEM),
        scratch_shapes=[
            vmem(rows, width),
            vmem(SIDE, rows, part),
            pltpu.VMEM((SIDE, 2, SIDE, 2 * rows), F32),
            pltpu.VMEM((SIDE, 2, SIDE, 2 * rows), F32),
            vmem(*blocks),
            vmem(*blocks),
            vmem(*blocks),
            vmem(2, part, hidden),
            vmem(2, part, hidden),
            vmem(2, hidden, part),
            pltpu.VMEM((SIDE, SIDE, cap, hidden), F32),
            pltpu.VMEM((SIDE, SIDE, cap, hidden), F32),
            vmem(SIDE, SIDE, cap, hidden),
            vmem(*blocks),
            vmem(*blocks),
            vmem(*blocks),
            vmem(*blocks),
            vmem(*blocks),
            vmem(SIDE, rows, part),
            vmem(SIDE, rows, part),
            dma((7,)),
        ]
        + [dma((SIDE,)) for _ in range(14)],
        compiler_params=pltpu.CompilerParams(
            collective_id=0, has_side_effects=True, vmem_limit_bytes=60 * 1024 * 1024
        ),
        name="moe",
    )(routes, tokens_in, norm_gain.reshape(1, width), gate_proj, up_proj, down_proj)


def solution(mesh):
    in_specs = (
        P(("grp", "ep"), None),
        P(),
        P("ep", None, "tp"),
        P("ep", None, "tp"),
        P("ep", "tp", None),
        P(("grp", "ep"), None),
        P(("grp", "ep"), None),
        P(("grp", "ep"), None),
    )
    out_specs = P(("grp", "ep"), "tp")
    return jax.shard_map(
        on_device, mesh=mesh, in_specs=in_specs, out_specs=out_specs, check_vma=False
    )
```

```python
import functools
import math

import jax
import jax.numpy as jnp
from jax import lax
from jax.experimental import pallas as pl
from jax.experimental.pallas import tpu as pltpu
from jax.sharding import PartitionSpec as P

TOP = 8
EXP_GRP = 8
EPSILON = 1e-06
MESH = pl.DeviceIdType.MESH
SIDE = 8
BF = jnp.bfloat16
F32 = jnp.float32

OFF = [0, 1, 7, 2, 6, 3, 5, 4]
BACK = [OFF.index((-o) % SIDE) for o in OFF]
FAR = SIDE - 1
OUTWARD = [
    ((0,), (), ()),
    ((1, 2), (), ()),
    ((3, 4), (0, 1), ()),
    ((5, 6), (2, 3), (0, 1)),
    ((FAR,), (4, 5, 6, FAR), (2, 3, 4, 5, 6, FAR)),
]
INWARD_GROUPS = [(FAR,), (5, 6), (3, 4), (1, 2), (0,)]
INWARD = [s for places in INWARD_GROUPS for s in places]
RING_CUT = 4
SUM_CUT = 2


def next_outward(place, p):
    if place + 2 < FAR:
        return place + 2
    return FAR if place == (6, 5)[p % 2] else None


def next_inward(place, p):
    if place == FAR:
        return ((5, 1), (6, 2))[p % 2]
    return {1: 0, 2: 6 + 1}.get(place, place - 2), 2 - place % 2


def sums_from(place, p):
    if place in (5, 6):
        return (place,) if place == (5, 6)[p % 2] else ()
    return {0: (0, 7), FAR: ()}.get(place, (place,))


def ring_offset(place):
    half = (place + 1) // 2
    odd = place % 2
    return (odd * half + (1 - odd) * (SIDE - half)) % SIDE


def moe_kernel(
    ids_ref, group_ref, weight_ref, tokens_hbm, gain_ref, gate_hbm, up_hbm, down_hbm, out_ref,
    tok_in, toks, meta_out, meta, sel, xin, xoth, wg, wu, wd, accg, accu, hid,
    part_out, part_own, part_in, res, ret, sums_out, sums_in, mixed,
    load_sem, ag_send, ag_recv, sum_send, sum_recv, meta_send, meta_recv, sel_send, xin_recv, xo_send, xo_recv,
    part_send, part_recv, res_send, ret_recv,
):
    rows, width = tok_in.shape
    part = width // 2
    cap = sel.shape[2]
    hidden = wg.shape[2]
    grp = lax.axis_index("grp")
    ep = lax.axis_index("ep")
    core = lax.axis_index("tp")
    up_y = ep // SIDE
    up_x = ep % SIDE
    first = up_x * (1 - core) + up_y * core
    second = up_y * (1 - core) + up_x * core
    step_first = (1 - core) + SIDE * core
    step_second = SIDE * (1 - core) + core

    def along_first(place):
        at = (first + OFF[place]) % SIDE
        return (grp, at * step_first + second * step_second, core)

    def along_second(place):
        at = (second + OFF[place]) % SIDE
        return (grp, first * step_first + at * step_second, core)

    partner = (grp, ep, 1 - core)

    barrier = pltpu.get_barrier_semaphore()
    for place in range(1, SIDE):
        pl.semaphore_signal(barrier, inc=1, device_id=along_first(place), device_id_type=MESH)
        pl.semaphore_signal(barrier, inc=1, device_id=along_second(place), device_id_type=MESH)
    pl.semaphore_signal(barrier, inc=1, device_id=partner, device_id_type=MESH)

    def send(src, dst, send_sem, recv_sem, to):
        copy = pltpu.make_async_remote_copy(
            src_ref=src, dst_ref=dst, send_sem=send_sem, recv_sem=recv_sem,
            device_id=to, device_id_type=MESH,
        )
        copy.start()

    def wait_bytes(ref, sem):
        pltpu.make_async_copy(ref, ref, sem).wait()

    own = pl.ds(pl.multiple_of(core * part, part), part)
    other = pl.ds(pl.multiple_of((1 - core) * part, part), part)
    tok_load = pltpu.make_async_copy(tokens_hbm, tok_in, load_sem.at[0])
    tok_load.start()
    loads = [
        pltpu.make_async_copy(gate_hbm.at[0, own], wg.at[0], load_sem.at[1]),
        pltpu.make_async_copy(up_hbm.at[0, own], wu.at[0], load_sem.at[2]),
        pltpu.make_async_copy(gate_hbm.at[0, other], wg.at[1], load_sem.at[3]),
        pltpu.make_async_copy(up_hbm.at[0, other], wu.at[1], load_sem.at[4]),
        pltpu.make_async_copy(down_hbm.at[0, :, own], wd.at[0], load_sem.at[5]),
        pltpu.make_async_copy(down_hbm.at[0, :, other], wd.at[1], load_sem.at[6]),
    ]
    for load in loads:
        load.start()

    lanes = 2 * rows
    experts = SIDE * SIDE
    row = lax.broadcasted_iota(jnp.int32, (experts, lanes), 0)
    lane = lax.broadcasted_iota(jnp.int32, (experts, lanes), 1)
    at_first = (first + ring_offset(row // SIDE)) % SIDE
    at_second = (second + ring_offset(row % SIDE)) % SIDE
    expert = at_first * step_first + at_second * step_second

    def across(ref):
        turned = ref[...].astype(F32)
        return jnp.concatenate([turned, turned], axis=1)

    ids, group_weights, weights = across(ids_ref), across(group_ref), across(weight_ref)
    weight_sum = jnp.sum(weights, axis=0, keepdims=True)
    named = jnp.zeros((experts, lanes), F32)
    weight = jnp.zeros((experts, lanes), F32)
    expert_f = expert.astype(F32)
    for k in range(TOP):
        match = expert_f == ids[k : k + 1, :]
        named = jnp.where(match, 1.0, named)
        weight = jnp.where(match, weights[k : k + 1, :], weight)
    group = expert // EXP_GRP
    group_part = jnp.zeros((experts, lanes), F32)
    for g in range(experts // EXP_GRP):
        group_part = jnp.where(group == g, group_weights[g : g + 1, :], group_part)
    gates = group_part * weight / weight_sum
    high = gates.astype(BF).astype(F32)
    gates = jnp.where(lane < rows, high, gates - high)
    before = lax.broadcasted_iota(jnp.int32, (lanes, lanes), 0)
    after = lax.broadcasted_iota(jnp.int32, (lanes, lanes), 1)
    earlier = jnp.where((before < after) & (before // rows == after // rows), 1.0, 0.0).astype(BF)
    rank = jnp.dot(named.astype(BF), earlier, preferred_element_type=F32)
    slots = jnp.where(named > 0.0, rank, -1.0)
    meta_out[:, 0] = slots.reshape(SIDE, SIDE, lanes)
    meta_out[:, 1] = gates.reshape(SIDE, SIDE, lanes)
    meta[0] = meta_out[0]

    tok_load.wait()
    values = tok_in[...].astype(F32)
    scale = lax.rsqrt(jnp.mean(values * values, axis=-1, keepdims=True) + EPSILON)
    toks[0] = (tok_in[:, own].astype(F32) * scale * gain_ref[:, own]).astype(BF)

    accg[...] = jnp.zeros_like(accg)
    accu[...] = jnp.zeros_like(accu)

    pl.semaphore_wait(barrier, 2 * (SIDE - 1) + 1)

    def piece(p):
        return pl.ds(p * (rows // RING_CUT), rows // RING_CUT)

    def pass_on(place, to_place, p):
        backward = place % 2 == 1 if place else to_place % 2 == 1
        send(
            toks.at[place, piece(p)], toks.at[to_place, piece(p)],
            ag_send.at[to_place, p], ag_recv.at[to_place, p], along_first(2 if backward else 1),
        )

    for place in range(1, SIDE):
        send(meta_out.at[place], meta.at[BACK[place]], meta_send.at[place], meta_recv.at[BACK[place]], along_first(place))
    for p in range(RING_CUT):
        pass_on(0, 1, p)
        pass_on(0, 2, p)

    slot_iota = (lax.broadcasted_iota(jnp.int32, (SIDE * cap, lanes), 0) % cap).astype(F32)

    def spread(table):
        return jnp.concatenate(
            [jnp.broadcast_to(table[j : j + 1, :], (cap, lanes)) for j in range(SIDE)], axis=0
        )

    def receive(places):
        for p in range(RING_CUT):
            for s in places:
                if s > 0:
                    wait_bytes(toks.at[s, piece(p)], ag_recv.at[s, p])
                    onward = next_outward(s, p)
                    if onward:
                        pass_on(s, onward, p)

    def pick_and_send(s):
        if s > 0:
            wait_bytes(meta.at[s], meta_recv.at[s])
        chosen = jnp.where(spread(meta[s, 0]) == slot_iota, 1.0, 0.0).astype(BF)[:, :rows]
        picked = jnp.dot(chosen, toks[s], preferred_element_type=F32).astype(BF)
        picked = picked.reshape(SIDE, cap, part)
        sel[s] = picked
        xin[s, 0] = picked[0]
        for place in range(SIDE - 1, 0, -1):
            send(sel.at[s, place], xin.at[s, BACK[place]], sel_send.at[s], xin_recv.at[s], along_second(place))

    def take_own(s):
        wait_bytes(xin.at[s, pl.ds(1, SIDE - 1)], xin_recv.at[s])
        send(xin.at[s], xoth.at[:, s], xo_send.at[s], xo_recv.at[s], partner)
        block = xin[s].reshape(SIDE * cap, part)
        accg[s] += jnp.dot(block, wg[0], preferred_element_type=F32).reshape(SIDE, cap, hidden)
        accu[s] += jnp.dot(block, wu[0], preferred_element_type=F32).reshape(SIDE, cap, hidden)

    def take_other(s):
        wait_bytes(xoth.at[:, s], xo_recv.at[s])
        block = xoth[:, s].reshape(SIDE * cap, part)
        accg[:, s] += jnp.dot(block, wg[1], preferred_element_type=F32).reshape(SIDE, cap, hidden)
        accu[:, s] += jnp.dot(block, wu[1], preferred_element_type=F32).reshape(SIDE, cap, hidden)

    for places, owns, others in OUTWARD:
        receive(places)
        for s in places:
            pick_and_send(s)
        if places == (3, 4):
            for load in loads:
                load.wait()
        for s in owns:
            take_own(s)
        for s in others:
            take_other(s)

    for s in range(SIDE):
        gate_acts = accg[s]
        hid[s] = (gate_acts / (1.0 + jnp.exp(-gate_acts)) * accu[s]).astype(BF)

    def multiply_down(s):
        theirs = hid[:, s].reshape(SIDE * cap, hidden)
        part_out[s] = jnp.dot(theirs, wd[1], preferred_element_type=F32).astype(BF).reshape(SIDE, cap, part)
        send(part_out.at[s], part_in.at[s], part_send.at[s], part_recv.at[s], partner)
        mine = hid[s].reshape(SIDE * cap, hidden)
        part_own[s] = jnp.dot(mine, wd[0], preferred_element_type=F32).astype(BF).reshape(SIDE, cap, part)

    def return_rows(s):
        wait_bytes(part_in.at[s], part_recv.at[s])
        res[s] = (part_own[s].astype(F32) + part_in[s].astype(F32)).astype(BF)
        ret[s, 0] = res[s, 0]
        for place in range(SIDE - 1, 0, -1):
            send(res.at[s, place], ret.at[s, BACK[place]], res_send.at[s], ret_recv.at[s], along_second(place))

    columns = part // SUM_CUT

    def mix(s, at):
        wait_bytes(ret.at[s, pl.ds(1, SIDE - 1)], ret_recv.at[s])
        mixer = jnp.where(spread(meta[s, 0]) == slot_iota, spread(meta[s, 1]), 0.0).astype(BF)
        both = lax.dot_general(
            mixer, ret[s].reshape(SIDE * cap, part), (((0,), (0,)), ((), ())), preferred_element_type=F32
        )
        mixed[at] = both[:rows] + both[rows:]

    def pass_sum(s, at, p):
        total = mixed[at, :, p * columns : (p + 1) * columns]
        for slot in sums_from(s, p):
            wait_bytes(sums_in.at[slot, p], sum_recv.at[slot, p])
            total = total + sums_in[slot, p].astype(F32)
        if s == 0:
            out_ref[:, p * columns : (p + 1) * columns] = total
            return
        sums_out[s, p] = total.astype(BF)
        to_slot, toward = next_inward(s, p)
        send(
            sums_out.at[s, p], sums_in.at[to_slot, p], sum_send.at[s, p], sum_recv.at[to_slot, p], along_first(toward)
        )

    for step in range(SIDE + 1):
        if step < SIDE:
            multiply_down(INWARD[step])
        if 1 <= step:
            return_rows(INWARD[step - 1])
    for places in INWARD_GROUPS:
        for at, s in enumerate(places):
            mix(s, at)
        for p in range(SUM_CUT):
            for at, s in enumerate(places):
                pass_sum(s, at, p)

    for place in range(1, SIDE):
        wait_bytes(meta_out.at[place], meta_send.at[place])
        for p in range(RING_CUT):
            wait_bytes(toks.at[place, piece(p)], ag_send.at[place, p])
        for p in range(SUM_CUT):
            wait_bytes(sums_out.at[place, p], sum_send.at[place, p])
    for s in range(SIDE):
        wait_bytes(sel.at[s, pl.ds(1, SIDE - 1)], sel_send.at[s])
        wait_bytes(xin.at[s], xo_send.at[s])
        wait_bytes(part_out.at[s], part_send.at[s])
        wait_bytes(res.at[s, pl.ds(1, SIDE - 1)], res_send.at[s])


def on_device(
    tokens_in, norm_gain, gate_proj, up_proj, down_proj, route_ids, group_weight, expert_weight
):
    rows, width = tokens_in.shape
    experts = gate_proj.shape[0] * lax.axis_size("ep")
    hidden = gate_proj.shape[2]
    cap = min(rows, max(2, 2 * rows * TOP // experts))
    part = width // 2
    vmem = lambda *shape: pltpu.VMEM(shape, BF)
    dma = pltpu.SemaphoreType.DMA
    blocks = (SIDE, SIDE, cap, part)
    result = pl.pallas_call(
        moe_kernel,
        out_shape=jax.ShapeDtypeStruct((rows, part), F32),
        in_specs=[
            pl.BlockSpec(memory_space=pltpu.VMEM),
            pl.BlockSpec(memory_space=pltpu.VMEM),
            pl.BlockSpec(memory_space=pltpu.VMEM),
            pl.BlockSpec(memory_space=pl.ANY),
            pl.BlockSpec(memory_space=pltpu.VMEM),
            pl.BlockSpec(memory_space=pl.ANY),
            pl.BlockSpec(memory_space=pl.ANY),
            pl.BlockSpec(memory_space=pl.ANY),
        ],
        out_specs=pl.BlockSpec(memory_space=pltpu.VMEM),
        scratch_shapes=[
            vmem(rows, width),
            vmem(SIDE, rows, part),
            pltpu.VMEM((SIDE, 2, SIDE, 2 * rows), F32),
            pltpu.VMEM((SIDE, 2, SIDE, 2 * rows), F32),
            vmem(*blocks),
            vmem(*blocks),
            vmem(*blocks),
            vmem(2, part, hidden),
            vmem(2, part, hidden),
            vmem(2, hidden, part),
            pltpu.VMEM((SIDE, SIDE, cap, hidden), F32),
            pltpu.VMEM((SIDE, SIDE, cap, hidden), F32),
            vmem(SIDE, SIDE, cap, hidden),
            vmem(*blocks),
            vmem(*blocks),
            vmem(*blocks),
            vmem(*blocks),
            vmem(*blocks),
            vmem(SIDE, SUM_CUT, rows, part // SUM_CUT),
            vmem(SIDE, SUM_CUT, rows, part // SUM_CUT),
            pltpu.VMEM((2, rows, part), F32),
            dma((7,)),
            dma((SIDE, RING_CUT)),
            dma((SIDE, RING_CUT)),
            dma((SIDE, SUM_CUT)),
            dma((SIDE, SUM_CUT)),
        ]
        + [dma((SIDE,)) for _ in range(10)],
        compiler_params=pltpu.CompilerParams(
            collective_id=0, has_side_effects=True, vmem_limit_bytes=60 * 1024 * 1024
        ),
        name="moe",
    )(
        route_ids.T, group_weight.T, expert_weight.T,
        tokens_in, norm_gain.reshape(1, width), gate_proj, up_proj, down_proj,
    )
    return result.astype(BF)


def solution(mesh):
    in_specs = (
        P(("grp", "ep"), None),
        P(),
        P("ep", None, "tp"),
        P("ep", None, "tp"),
        P("ep", "tp", None),
        P(("grp", "ep"), None),
        P(("grp", "ep"), None),
        P(("grp", "ep"), None),
    )
    out_specs = P(("grp", "ep"), "tp")
    return jax.shard_map(
        on_device, mesh=mesh, in_specs=in_specs, out_specs=out_specs, check_vma=False
    )
```

```python
import functools
import math

import jax
import jax.numpy as jnp
from jax import lax
from jax.experimental import pallas as pl
from jax.experimental.pallas import tpu as pltpu
from jax.sharding import PartitionSpec as P

TOP = 8
EXP_GRP = 8
EPSILON = 1e-06
MESH = pl.DeviceIdType.MESH
SIDE = 8
BF = jnp.bfloat16
F32 = jnp.float32

OFF = [0, 1, 7, 2, 6, 3, 5, 4]
BACK = [OFF.index((-o) % SIDE) for o in OFF]
FAR = SIDE - 1
INWARD_GROUPS = [(FAR,), (5, 6), (3, 4), (1, 2), (0,)]
INWARD = [s for places in INWARD_GROUPS for s in places]
RING_CUT = 4
SUM_CUT = 2


def next_outward(place, p):
    if place + 2 < FAR:
        return place + 2
    return FAR if place == (6, 5)[p % 2] else None


def next_inward(place, p):
    if place == FAR:
        return ((5, 1), (6, 2))[p % 2]
    return {1: 0, 2: 6 + 1}.get(place, place - 2), 2 - place % 2


def sums_from(place, p):
    if place in (5, 6):
        return (place,) if place == (5, 6)[p % 2] else ()
    return {0: (0, 7), FAR: ()}.get(place, (place,))


def ring_offset(place):
    half = (place + 1) // 2
    odd = place % 2
    return (odd * half + (1 - odd) * (SIDE - half)) % SIDE


def moe_kernel(
    ids_ref, group_ref, weight_ref, tokens_hbm, gain_ref, gate_hbm, up_hbm, down_hbm, out_ref,
    tok_in, toks, meta_out, meta, sel, xin, xoth, wg, wu, wd, accg, accu, hid,
    part_out, part_own, part_in, res, ret, sums_out, sums_in, mixed,
    load_sem, ag_send, ag_recv, sum_send, sum_recv, meta_send, meta_recv, sel_send, xin_recv, xo_send, xo_recv,
    part_send, part_recv, res_send, ret_recv, lead_sem,
):
    rows, width = tok_in.shape
    part = width // 2
    cap = sel.shape[2]
    hidden = wg.shape[2]
    grp = lax.axis_index("grp")
    ep = lax.axis_index("ep")
    core = lax.axis_index("tp")
    up_y = ep // SIDE
    up_x = ep % SIDE
    first = up_x * (1 - core) + up_y * core
    second = up_y * (1 - core) + up_x * core
    step_first = (1 - core) + SIDE * core
    step_second = SIDE * (1 - core) + core

    def along_first(place):
        at = (first + OFF[place]) % SIDE
        return (grp, at * step_first + second * step_second, core)

    def along_second(place):
        at = (second + OFF[place]) % SIDE
        return (grp, first * step_first + at * step_second, core)

    partner = (grp, ep, 1 - core)

    peer_count = 2 * (SIDE - 1) + 1
    in_lead_row = (second == 0) & (core == 0)
    in_lead_column = (first == 0) & (core == 0)
    is_lead = in_lead_row & in_lead_column
    beside_lead = (ep == 0) & (core == 1)
    knows_lead = (in_lead_row | in_lead_column | beside_lead) & jnp.logical_not(is_lead)

    def signal_peers(semaphore):
        for place in range(1, SIDE):
            pl.semaphore_signal(semaphore, inc=1, device_id=along_first(place), device_id_type=MESH)
            pl.semaphore_signal(semaphore, inc=1, device_id=along_second(place), device_id_type=MESH)
        pl.semaphore_signal(semaphore, inc=1, device_id=partner, device_id_type=MESH)

    barrier = pltpu.get_barrier_semaphore()

    @pl.when(jnp.logical_not(is_lead))
    def _():
        signal_peers(barrier)

    def await_lead(who):
        @pl.when(who & jnp.logical_not(is_lead))
        def _():
            pl.semaphore_wait(lead_sem, 1)

    def send(src, dst, send_sem, recv_sem, to):
        copy = pltpu.make_async_remote_copy(
            src_ref=src, dst_ref=dst, send_sem=send_sem, recv_sem=recv_sem,
            device_id=to, device_id_type=MESH,
        )
        copy.start()

    def wait_bytes(ref, sem):
        pltpu.make_async_copy(ref, ref, sem).wait()

    own = pl.ds(pl.multiple_of(core * part, part), part)
    other = pl.ds(pl.multiple_of((1 - core) * part, part), part)
    tok_load = pltpu.make_async_copy(tokens_hbm, tok_in, load_sem.at[0])
    tok_load.start()
    loads = [
        pltpu.make_async_copy(gate_hbm.at[0, own], wg.at[0], load_sem.at[1]),
        pltpu.make_async_copy(up_hbm.at[0, own], wu.at[0], load_sem.at[2]),
        pltpu.make_async_copy(gate_hbm.at[0, other], wg.at[1], load_sem.at[3]),
        pltpu.make_async_copy(up_hbm.at[0, other], wu.at[1], load_sem.at[4]),
        pltpu.make_async_copy(down_hbm.at[0, :, own], wd.at[0], load_sem.at[5]),
        pltpu.make_async_copy(down_hbm.at[0, :, other], wd.at[1], load_sem.at[6]),
    ]
    for load in loads:
        load.start()

    tok_load.wait()
    values = tok_in[...].astype(F32)
    scale = lax.rsqrt(jnp.mean(values * values, axis=-1, keepdims=True) + EPSILON)
    toks[0] = (tok_in[:, own].astype(F32) * scale * gain_ref[:, own]).astype(BF)

    pl.semaphore_wait(barrier, peer_count - knows_lead.astype(jnp.int32))

    @pl.when(is_lead)
    def _():
        signal_peers(lead_sem)

    await_lead(in_lead_row)

    def piece(p):
        return pl.ds(p * (rows // RING_CUT), rows // RING_CUT)

    def pass_on(place, to_place, p):
        backward = place % 2 == 1 if place else to_place % 2 == 1
        send(
            toks.at[place, piece(p)], toks.at[to_place, piece(p)],
            ag_send.at[to_place, p], ag_recv.at[to_place, p], along_first(2 if backward else 1),
        )

    for p in range(RING_CUT):
        pass_on(0, 1, p)
        pass_on(0, 2, p)

    lanes = 2 * rows
    experts = SIDE * SIDE
    row = lax.broadcasted_iota(jnp.int32, (experts, lanes), 0)
    lane = lax.broadcasted_iota(jnp.int32, (experts, lanes), 1)
    at_first = (first + ring_offset(row // SIDE)) % SIDE
    at_second = (second + ring_offset(row % SIDE)) % SIDE
    expert = at_first * step_first + at_second * step_second

    def across(ref):
        turned = ref[...].astype(F32)
        return jnp.concatenate([turned, turned], axis=1)

    ids, group_weights, weights = across(ids_ref), across(group_ref), across(weight_ref)
    weight_sum = jnp.sum(weights, axis=0, keepdims=True)
    named = jnp.zeros((experts, lanes), F32)
    weight = jnp.zeros((experts, lanes), F32)
    expert_f = expert.astype(F32)
    for k in range(TOP):
        match = expert_f == ids[k : k + 1, :]
        named = jnp.where(match, 1.0, named)
        weight = jnp.where(match, weights[k : k + 1, :], weight)
    group = expert // EXP_GRP
    group_part = jnp.zeros((experts, lanes), F32)
    for g in range(experts // EXP_GRP):
        group_part = jnp.where(group == g, group_weights[g : g + 1, :], group_part)
    gates = group_part * weight / weight_sum
    high = gates.astype(BF).astype(F32)
    gates = jnp.where(lane < rows, high, gates - high)
    before = lax.broadcasted_iota(jnp.int32, (lanes, lanes), 0)
    after = lax.broadcasted_iota(jnp.int32, (lanes, lanes), 1)
    earlier = jnp.where((before < after) & (before // rows == after // rows), 1.0, 0.0).astype(BF)
    rank = jnp.dot(named.astype(BF), earlier, preferred_element_type=F32)
    slots = jnp.where(named > 0.0, rank, -1.0)
    meta_out[:, 0] = slots.reshape(SIDE, SIDE, lanes)
    meta_out[:, 1] = gates.reshape(SIDE, SIDE, lanes)
    meta[0] = meta_out[0]

    for place in range(1, SIDE):
        send(meta_out.at[place], meta.at[BACK[place]], meta_send.at[place], meta_recv.at[BACK[place]], along_first(place))
    accg[...] = jnp.zeros_like(accg)
    accu[...] = jnp.zeros_like(accu)

    slot_iota = (lax.broadcasted_iota(jnp.int32, (SIDE * cap, lanes), 0) % cap).astype(F32)

    def spread(table):
        return jnp.concatenate(
            [jnp.broadcast_to(table[j : j + 1, :], (cap, lanes)) for j in range(SIDE)], axis=0
        )

    def receive(places):
        for p in range(RING_CUT):
            for s in places:
                if s > 0:
                    wait_bytes(toks.at[s, piece(p)], ag_recv.at[s, p])
                    onward = next_outward(s, p)
                    if onward:
                        pass_on(s, onward, p)

    up = (SIDE - second) % SIDE
    beyond = up // (SIDE // 2 + 1)
    lead_place = (1 - beyond) * (2 * up - 1) + beyond * 2 * (SIDE - up)
    my_place = lead_place + 2 * (lead_place % 2) - 1 - lead_place // FAR
    follows = (in_lead_column & jnp.logical_not(is_lead)).astype(jnp.int32)
    lead_place = lead_place * follows - (1 - follows)

    def pick_and_send(s):
        if s > 0:
            wait_bytes(meta.at[s], meta_recv.at[s])
        chosen = jnp.where(spread(meta[s, 0]) == slot_iota, 1.0, 0.0).astype(BF)[:, :rows]
        picked = jnp.dot(chosen, toks[s], preferred_element_type=F32).astype(BF)
        picked = picked.reshape(SIDE, cap, part)
        sel[s] = picked
        xin[s, 0] = picked[0]
        for place in range(SIDE - 1, 0, -1):

            @pl.when(place != lead_place)
            def _():
                send(sel.at[s, place], xin.at[s, BACK[place]], sel_send.at[s], xin_recv.at[s], along_second(place))

    def take_own(s):
        wait_bytes(xin.at[s, pl.ds(1, SIDE - 1)], xin_recv.at[s])
        send(xin.at[s], xoth.at[:, s], xo_send.at[s], xo_recv.at[s], partner)
        block = xin[s].reshape(SIDE * cap, part)
        accg[s] += jnp.dot(block, wg[0], preferred_element_type=F32).reshape(SIDE, cap, hidden)
        accu[s] += jnp.dot(block, wu[0], preferred_element_type=F32).reshape(SIDE, cap, hidden)

    def take_other(s):
        wait_bytes(xoth.at[:, s], xo_recv.at[s])
        block = xoth[:, s].reshape(SIDE * cap, part)
        accg[:, s] += jnp.dot(block, wg[1], preferred_element_type=F32).reshape(SIDE, cap, hidden)
        accu[:, s] += jnp.dot(block, wu[1], preferred_element_type=F32).reshape(SIDE, cap, hidden)

    def activate(*at):
        gate_acts = accg[at]
        hid[at] = (gate_acts / (1.0 + jnp.exp(-gate_acts)) * accu[at]).astype(BF)

    receive((1, 2))
    for s in (0, 1, 2):
        pick_and_send(s)
    for places in ((3, 4), (5, 6), (FAR,)):
        receive(places)
        for s in places:
            pick_and_send(s)
    await_lead(in_lead_column)

    @pl.when(lead_place > 0)
    def _():
        for s in range(SIDE):
            send(sel.at[s, lead_place], xin.at[s, my_place], sel_send.at[s], xin_recv.at[s], (grp, 0, core))

    for load in loads:
        load.wait()
    await_lead(beside_lead)
    take_own(0)
    for s in range(1, FAR):
        take_own(s)
        take_other(s - 1)
    take_other(FAR - 1)
    for s in range(FAR):
        activate(s, pl.ds(0, FAR))
    take_own(FAR)
    take_other(FAR)
    activate(FAR)
    activate(pl.ds(0, FAR), FAR)

    def multiply_down(s):
        theirs = hid[:, s].reshape(SIDE * cap, hidden)
        part_out[s] = jnp.dot(theirs, wd[1], preferred_element_type=F32).astype(BF).reshape(SIDE, cap, part)
        send(part_out.at[s], part_in.at[s], part_send.at[s], part_recv.at[s], partner)
        mine = hid[s].reshape(SIDE * cap, hidden)
        part_own[s] = jnp.dot(mine, wd[0], preferred_element_type=F32).astype(BF).reshape(SIDE, cap, part)

    def return_rows(s):
        wait_bytes(part_in.at[s], part_recv.at[s])
        res[s] = (part_own[s].astype(F32) + part_in[s].astype(F32)).astype(BF)
        ret[s, 0] = res[s, 0]
        for place in range(SIDE - 1, 0, -1):
            send(res.at[s, place], ret.at[s, BACK[place]], res_send.at[s], ret_recv.at[s], along_second(place))

    columns = part // SUM_CUT

    def mix(s, at):
        wait_bytes(ret.at[s, pl.ds(1, SIDE - 1)], ret_recv.at[s])
        mixer = jnp.where(spread(meta[s, 0]) == slot_iota, spread(meta[s, 1]), 0.0).astype(BF)
        both = lax.dot_general(
            mixer, ret[s].reshape(SIDE * cap, part), (((0,), (0,)), ((), ())), preferred_element_type=F32
        )
        mixed[at] = both[:rows] + both[rows:]

    def pass_sum(s, at, p):
        total = mixed[at, :, p * columns : (p + 1) * columns]
        for slot in sums_from(s, p):
            wait_bytes(sums_in.at[slot, p], sum_recv.at[slot, p])
            total = total + sums_in[slot, p].astype(F32)
        if s == 0:
            out_ref[:, p * columns : (p + 1) * columns] = total
            return
        sums_out[s, p] = total.astype(BF)
        to_slot, toward = next_inward(s, p)
        send(
            sums_out.at[s, p], sums_in.at[to_slot, p], sum_send.at[s, p], sum_recv.at[to_slot, p], along_first(toward)
        )

    for step in range(SIDE + 1):
        if step < SIDE:
            multiply_down(INWARD[step])
        if 1 <= step:
            return_rows(INWARD[step - 1])
    for places in INWARD_GROUPS:
        for at, s in enumerate(places):
            mix(s, at)
        for p in range(SUM_CUT):
            for at, s in enumerate(places):
                pass_sum(s, at, p)

    for place in range(1, SIDE):
        wait_bytes(meta_out.at[place], meta_send.at[place])
        for p in range(RING_CUT):
            wait_bytes(toks.at[place, piece(p)], ag_send.at[place, p])
        for p in range(SUM_CUT):
            wait_bytes(sums_out.at[place, p], sum_send.at[place, p])
    for s in range(SIDE):
        wait_bytes(sel.at[s, pl.ds(1, SIDE - 1)], sel_send.at[s])
        wait_bytes(xin.at[s], xo_send.at[s])
        wait_bytes(part_out.at[s], part_send.at[s])
        wait_bytes(res.at[s, pl.ds(1, SIDE - 1)], res_send.at[s])


def on_device(
    tokens_in, norm_gain, gate_proj, up_proj, down_proj, route_ids, group_weight, expert_weight
):
    rows, width = tokens_in.shape
    experts = gate_proj.shape[0] * lax.axis_size("ep")
    hidden = gate_proj.shape[2]
    cap = min(rows, max(2, 2 * rows * TOP // experts))
    part = width // 2
    vmem = lambda *shape: pltpu.VMEM(shape, BF)
    dma = pltpu.SemaphoreType.DMA
    blocks = (SIDE, SIDE, cap, part)
    result = pl.pallas_call(
        moe_kernel,
        out_shape=jax.ShapeDtypeStruct((rows, part), F32),
        in_specs=[
            pl.BlockSpec(memory_space=pltpu.VMEM),
            pl.BlockSpec(memory_space=pltpu.VMEM),
            pl.BlockSpec(memory_space=pltpu.VMEM),
            pl.BlockSpec(memory_space=pl.ANY),
            pl.BlockSpec(memory_space=pltpu.VMEM),
            pl.BlockSpec(memory_space=pl.ANY),
            pl.BlockSpec(memory_space=pl.ANY),
            pl.BlockSpec(memory_space=pl.ANY),
        ],
        out_specs=pl.BlockSpec(memory_space=pltpu.VMEM),
        scratch_shapes=[
            vmem(rows, width),
            vmem(SIDE, rows, part),
            pltpu.VMEM((SIDE, 2, SIDE, 2 * rows), F32),
            pltpu.VMEM((SIDE, 2, SIDE, 2 * rows), F32),
            vmem(*blocks),
            vmem(*blocks),
            vmem(*blocks),
            vmem(2, part, hidden),
            vmem(2, part, hidden),
            vmem(2, hidden, part),
            pltpu.VMEM((SIDE, SIDE, cap, hidden), F32),
            pltpu.VMEM((SIDE, SIDE, cap, hidden), F32),
            vmem(SIDE, SIDE, cap, hidden),
            vmem(*blocks),
            vmem(*blocks),
            vmem(*blocks),
            vmem(*blocks),
            vmem(*blocks),
            vmem(SIDE, SUM_CUT, rows, part // SUM_CUT),
            vmem(SIDE, SUM_CUT, rows, part // SUM_CUT),
            pltpu.VMEM((2, rows, part), F32),
            dma((7,)),
            dma((SIDE, RING_CUT)),
            dma((SIDE, RING_CUT)),
            dma((SIDE, SUM_CUT)),
            dma((SIDE, SUM_CUT)),
        ]
        + [dma((SIDE,)) for _ in range(10)]
        + [pltpu.SemaphoreType.REGULAR],
        compiler_params=pltpu.CompilerParams(
            collective_id=0, has_side_effects=True, vmem_limit_bytes=60 * 1024 * 1024
        ),
        name="moe",
    )(
        route_ids.T, group_weight.T, expert_weight.T,
        tokens_in, norm_gain.reshape(1, width), gate_proj, up_proj, down_proj,
    )
    return result.astype(BF)


def solution(mesh):
    in_specs = (
        P(("grp", "ep"), None),
        P(),
        P("ep", None, "tp"),
        P("ep", None, "tp"),
        P("ep", "tp", None),
        P(("grp", "ep"), None),
        P(("grp", "ep"), None),
        P(("grp", "ep"), None),
    )
    out_specs = P(("grp", "ep"), "tp")
    return jax.shard_map(
        on_device, mesh=mesh, in_specs=in_specs, out_specs=out_specs, check_vma=False
    )
```

```python
import functools
import math

import jax
import jax.numpy as jnp
from jax import lax
from jax.experimental import pallas as pl
from jax.experimental.pallas import tpu as pltpu
from jax.sharding import PartitionSpec as P

TOP = 8
EXP_GRP = 8
EPSILON = 1e-06
MESH = pl.DeviceIdType.MESH
SIDE = 8
BF = jnp.bfloat16
F32 = jnp.float32

OFF = [0, 1, 7, 2, 6, 3, 5, 4]
BACK = [OFF.index((-o) % SIDE) for o in OFF]
FAR = SIDE - 1
INWARD_GROUPS = [(FAR,), (5, 6), (3, 4), (1, 2), (0,)]
INWARD = [s for places in INWARD_GROUPS for s in places]
RING_CUT = 4
SUM_CUT = 2
HELD_BACK = 5


def next_outward(place, p):
    if place + 2 < FAR:
        return place + 2
    return FAR if place == (6, 5)[p % 2] else None


def next_inward(place, p):
    if place == FAR:
        return ((5, 1), (6, 2))[p % 2]
    return {1: 0, 2: 6 + 1}.get(place, place - 2), 2 - place % 2


def sums_from(place, p):
    if place in (5, 6):
        return (place,) if place == (5, 6)[p % 2] else ()
    return {0: (0, 7), FAR: ()}.get(place, (place,))


def ring_offset(place):
    half = (place + 1) // 2
    odd = place % 2
    return (odd * half + (1 - odd) * (SIDE - half)) % SIDE


def moe_kernel(
    ids_ref, group_ref, weight_ref, tokens_hbm, gain_ref, gate_hbm, up_hbm, down_hbm, out_ref,
    tok_in, toks, meta_out, meta, sel, xin, xoth, wg, wu, wd, accg, accu, hid,
    part_out, part_own, part_in, res, ret, sums_out, sums_in, mixed,
    load_sem, ag_send, ag_recv, sum_send, sum_recv, meta_send, meta_recv, sel_send, xin_recv, xo_send, xo_recv,
    part_send, part_recv, res_send, ret_recv, lead_sem,
):
    rows, width = tok_in.shape
    part = width // 2
    cap = sel.shape[2]
    hidden = wg.shape[2]
    grp = lax.axis_index("grp")
    ep = lax.axis_index("ep")
    core = lax.axis_index("tp")
    up_y = ep // SIDE
    up_x = ep % SIDE
    first = up_x * (1 - core) + up_y * core
    second = up_y * (1 - core) + up_x * core
    step_first = (1 - core) + SIDE * core
    step_second = SIDE * (1 - core) + core

    def along_first(place):
        at = (first + OFF[place]) % SIDE
        return (grp, at * step_first + second * step_second, core)

    def along_second(place):
        at = (second + OFF[place]) % SIDE
        return (grp, first * step_first + at * step_second, core)

    partner = (grp, ep, 1 - core)

    peer_count = 2 * (SIDE - 1) + 1
    in_lead_row = (second == 0) & (core == 0)
    in_lead_column = (first == 0) & (core == 0)
    is_lead = in_lead_row & in_lead_column
    beside_lead = (ep == 0) & (core == 1)
    knows_lead = (in_lead_row | in_lead_column | beside_lead) & jnp.logical_not(is_lead)

    def signal_peers(semaphore):
        for place in range(1, SIDE):
            pl.semaphore_signal(semaphore, inc=1, device_id=along_first(place), device_id_type=MESH)
            pl.semaphore_signal(semaphore, inc=1, device_id=along_second(place), device_id_type=MESH)
        pl.semaphore_signal(semaphore, inc=1, device_id=partner, device_id_type=MESH)

    barrier = pltpu.get_barrier_semaphore()

    @pl.when(jnp.logical_not(is_lead))
    def _():
        signal_peers(barrier)

    def await_lead(who):
        @pl.when(who & jnp.logical_not(is_lead))
        def _():
            pl.semaphore_wait(lead_sem, 1)

    def send(src, dst, send_sem, recv_sem, to):
        copy = pltpu.make_async_remote_copy(
            src_ref=src, dst_ref=dst, send_sem=send_sem, recv_sem=recv_sem,
            device_id=to, device_id_type=MESH,
        )
        copy.start()

    def wait_bytes(ref, sem):
        pltpu.make_async_copy(ref, ref, sem).wait()

    own = pl.ds(pl.multiple_of(core * part, part), part)
    other = pl.ds(pl.multiple_of((1 - core) * part, part), part)
    tok_load = pltpu.make_async_copy(tokens_hbm, tok_in, load_sem.at[0])
    tok_load.start()
    loads = [
        pltpu.make_async_copy(gate_hbm.at[0, own], wg.at[0], load_sem.at[1]),
        pltpu.make_async_copy(up_hbm.at[0, own], wu.at[0], load_sem.at[2]),
        pltpu.make_async_copy(gate_hbm.at[0, other], wg.at[1], load_sem.at[3]),
        pltpu.make_async_copy(up_hbm.at[0, other], wu.at[1], load_sem.at[4]),
        pltpu.make_async_copy(down_hbm.at[0, :, own], wd.at[0], load_sem.at[5]),
        pltpu.make_async_copy(down_hbm.at[0, :, other], wd.at[1], load_sem.at[6]),
    ]
    for load in loads:
        load.start()

    tok_load.wait()
    values = tok_in[...].astype(F32)
    scale = lax.rsqrt(jnp.mean(values * values, axis=-1, keepdims=True) + EPSILON)
    toks[0] = (tok_in[:, own].astype(F32) * scale * gain_ref[:, own]).astype(BF)

    pl.semaphore_wait(barrier, peer_count - knows_lead.astype(jnp.int32))

    @pl.when(is_lead)
    def _():
        signal_peers(lead_sem)

    await_lead(in_lead_row)

    def piece(p):
        return pl.ds(p * (rows // RING_CUT), rows // RING_CUT)

    def pass_on(place, to_place, p):
        backward = place % 2 == 1 if place else to_place % 2 == 1
        send(
            toks.at[place, piece(p)], toks.at[to_place, piece(p)],
            ag_send.at[to_place, p], ag_recv.at[to_place, p], along_first(2 if backward else 1),
        )

    for p in range(RING_CUT):
        pass_on(0, 1, p)
        pass_on(0, 2, p)

    lanes = 2 * rows
    experts = SIDE * SIDE
    row = lax.broadcasted_iota(jnp.int32, (experts, lanes), 0)
    lane = lax.broadcasted_iota(jnp.int32, (experts, lanes), 1)
    at_first = (first + ring_offset(row // SIDE)) % SIDE
    at_second = (second + ring_offset(row % SIDE)) % SIDE
    expert = at_first * step_first + at_second * step_second

    def across(ref):
        turned = ref[...].astype(F32)
        return jnp.concatenate([turned, turned], axis=1)

    ids, group_weights, weights = across(ids_ref), across(group_ref), across(weight_ref)
    weight_sum = jnp.sum(weights, axis=0, keepdims=True)
    named = jnp.zeros((experts, lanes), F32)
    weight = jnp.zeros((experts, lanes), F32)
    expert_f = expert.astype(F32)
    for k in range(TOP):
        match = expert_f == ids[k : k + 1, :]
        named = jnp.where(match, 1.0, named)
        weight = jnp.where(match, weights[k : k + 1, :], weight)
    group = expert // EXP_GRP
    group_part = jnp.zeros((experts, lanes), F32)
    for g in range(experts // EXP_GRP):
        group_part = jnp.where(group == g, group_weights[g : g + 1, :], group_part)
    gates = group_part * weight / weight_sum
    high = gates.astype(BF).astype(F32)
    gates = jnp.where(lane < rows, high, gates - high)
    before = lax.broadcasted_iota(jnp.int32, (lanes, lanes), 0)
    after = lax.broadcasted_iota(jnp.int32, (lanes, lanes), 1)
    earlier = jnp.where((before < after) & (before // rows == after // rows), 1.0, 0.0).astype(BF)
    rank = jnp.dot(named.astype(BF), earlier, preferred_element_type=F32)
    slots = jnp.where(named > 0.0, rank, -1.0)
    meta_out[:, 0] = slots.reshape(SIDE, SIDE, lanes)
    meta_out[:, 1] = gates.reshape(SIDE, SIDE, lanes)
    meta[0] = meta_out[0]

    for place in range(1, SIDE):
        send(meta_out.at[place], meta.at[BACK[place]], meta_send.at[place], meta_recv.at[BACK[place]], along_first(place))
    accg[...] = jnp.zeros_like(accg)
    accu[...] = jnp.zeros_like(accu)

    slot_iota = (lax.broadcasted_iota(jnp.int32, (SIDE * cap, lanes), 0) % cap).astype(F32)

    def spread(table):
        return jnp.concatenate(
            [jnp.broadcast_to(table[j : j + 1, :], (cap, lanes)) for j in range(SIDE)], axis=0
        )

    def receive(places):
        for p in range(RING_CUT):
            for s in places:
                if s > 0:
                    wait_bytes(toks.at[s, piece(p)], ag_recv.at[s, p])
                    onward = next_outward(s, p)
                    if onward:
                        pass_on(s, onward, p)

    up = (SIDE - second) % SIDE
    beyond = up // (SIDE // 2 + 1)
    lead_place = (1 - beyond) * (2 * up - 1) + beyond * 2 * (SIDE - up)
    my_place = lead_place + 2 * (lead_place % 2) - 1 - lead_place // FAR
    follows = (in_lead_column & jnp.logical_not(is_lead)).astype(jnp.int32)
    lead_place = lead_place * follows - (1 - follows)
    lead = (grp, 0, core)

    def pick_and_send(s):
        if s > 0:
            wait_bytes(meta.at[s], meta_recv.at[s])
        chosen = jnp.where(spread(meta[s, 0]) == slot_iota, 1.0, 0.0).astype(BF)[:, :rows]
        picked = jnp.dot(chosen, toks[s], preferred_element_type=F32).astype(BF)
        picked = picked.reshape(SIDE, cap, part)
        sel[s] = picked
        xin[s, 0] = picked[0]
        for place in range(SIDE - 1, 0, -1):

            def send_rows():
                send(sel.at[s, place], xin.at[s, BACK[place]], sel_send.at[s], xin_recv.at[s], along_second(place))

            if s < HELD_BACK:
                pl.when(place != lead_place)(send_rows)
            else:
                send_rows()

    def multiply_in(block, at, half):
        for acc, weights in ((accg, wg), (accu, wu)):
            acts = jnp.dot(block.reshape(-1, part), weights[half], preferred_element_type=F32)
            acc[at] += acts.reshape(block.shape[:-1] + (hidden,))

    def take_own(s, count=1):
        for one in range(s, s + count):
            wait_bytes(xin.at[one, pl.ds(1, SIDE - 1)], xin_recv.at[one])
            send(xin.at[one], xoth.at[:, one], xo_send.at[one], xo_recv.at[one], partner)
        multiply_in(xin[s : s + count], (pl.ds(s, count),), 0)

    def take_other(s, count=1):
        for one in range(s, s + count):
            wait_bytes(xoth.at[:, one], xo_recv.at[one])
        multiply_in(xoth[:, s : s + count], (slice(None), pl.ds(s, count)), 1)

    def activate(*at):
        gate_acts = accg[at]
        hid[at] = (gate_acts / (1.0 + jnp.exp(-gate_acts)) * accu[at]).astype(BF)

    early = in_lead_row & jnp.logical_not(is_lead)

    def when(condition, *work):
        @pl.when(condition)
        def _():
            for take, s in work:
                take(s, 2)

    receive((1, 2))
    for s in (0, 1, 2):
        pick_and_send(s)
    receive((3, 4))
    for s in (3, 4):
        pick_and_send(s)
    await_lead(in_lead_column)

    @pl.when(lead_place > 0)
    def _():
        for s in range(HELD_BACK):
            send(sel.at[s, lead_place], xin.at[s, my_place], sel_send.at[s], xin_recv.at[s], lead)

    for load in loads:
        load.wait()
    when(early, (take_own, 0))
    receive((5, 6))
    for s in (5, 6):
        pick_and_send(s)
    when(early, (take_own, 2), (take_other, 0))
    when(is_lead, (take_own, 0))
    receive((FAR,))
    pick_and_send(FAR)
    await_lead(beside_lead)
    when(jnp.logical_not(in_lead_row), (take_own, 0))
    when(jnp.logical_not(early), (take_own, 2), (take_other, 0))
    take_own(4, 2)
    take_other(2, 2)
    take_own(FAR - 1)
    take_other(4, 2)
    take_other(FAR - 1)
    take_own(FAR)
    for s in range(FAR):
        activate(s, pl.ds(0, FAR))
    take_other(FAR)
    activate(FAR)
    activate(pl.ds(0, FAR), FAR)

    def multiply_down(s):
        theirs = hid[:, s].reshape(SIDE * cap, hidden)
        part_out[s] = jnp.dot(theirs, wd[1], preferred_element_type=F32).astype(BF).reshape(SIDE, cap, part)
        send(part_out.at[s], part_in.at[s], part_send.at[s], part_recv.at[s], partner)
        mine = hid[s].reshape(SIDE * cap, hidden)
        part_own[s] = jnp.dot(mine, wd[0], preferred_element_type=F32).astype(BF).reshape(SIDE, cap, part)

    def return_rows(s):
        wait_bytes(part_in.at[s], part_recv.at[s])
        res[s] = (part_own[s].astype(F32) + part_in[s].astype(F32)).astype(BF)
        ret[s, 0] = res[s, 0]
        for place in range(SIDE - 1, 0, -1):
            send(res.at[s, place], ret.at[s, BACK[place]], res_send.at[s], ret_recv.at[s], along_second(place))

    columns = part // SUM_CUT

    def mix(s, at):
        wait_bytes(ret.at[s, pl.ds(1, SIDE - 1)], ret_recv.at[s])
        mixer = jnp.where(spread(meta[s, 0]) == slot_iota, spread(meta[s, 1]), 0.0).astype(BF)
        both = lax.dot_general(
            mixer, ret[s].reshape(SIDE * cap, part), (((0,), (0,)), ((), ())), preferred_element_type=F32
        )
        mixed[at] = both[:rows] + both[rows:]

    def pass_sum(s, at, p):
        total = mixed[at, :, p * columns : (p + 1) * columns]
        for slot in sums_from(s, p):
            wait_bytes(sums_in.at[slot, p], sum_recv.at[slot, p])
            total = total + sums_in[slot, p].astype(F32)
        if s == 0:
            out_ref[:, p * columns : (p + 1) * columns] = total
            return
        sums_out[s, p] = total.astype(BF)
        to_slot, toward = next_inward(s, p)
        send(
            sums_out.at[s, p], sums_in.at[to_slot, p], sum_send.at[s, p], sum_recv.at[to_slot, p], along_first(toward)
        )

    for step in range(SIDE + 1):
        if step < SIDE:
            multiply_down(INWARD[step])
        if 1 <= step:
            return_rows(INWARD[step - 1])
    for places in INWARD_GROUPS:
        for at, s in enumerate(places):
            mix(s, at)
        for p in range(SUM_CUT):
            for at, s in enumerate(places):
                pass_sum(s, at, p)

    for place in range(1, SIDE):
        wait_bytes(meta_out.at[place], meta_send.at[place])
        for p in range(RING_CUT):
            wait_bytes(toks.at[place, piece(p)], ag_send.at[place, p])
        for p in range(SUM_CUT):
            wait_bytes(sums_out.at[place, p], sum_send.at[place, p])
    for s in range(SIDE):
        wait_bytes(sel.at[s, pl.ds(1, SIDE - 1)], sel_send.at[s])
        wait_bytes(xin.at[s], xo_send.at[s])
        wait_bytes(part_out.at[s], part_send.at[s])
        wait_bytes(res.at[s, pl.ds(1, SIDE - 1)], res_send.at[s])


def on_device(
    tokens_in, norm_gain, gate_proj, up_proj, down_proj, route_ids, group_weight, expert_weight
):
    rows, width = tokens_in.shape
    experts = gate_proj.shape[0] * lax.axis_size("ep")
    hidden = gate_proj.shape[2]
    cap = min(rows, max(2, 2 * rows * TOP // experts))
    part = width // 2
    vmem = lambda *shape: pltpu.VMEM(shape, BF)
    dma = pltpu.SemaphoreType.DMA
    blocks = (SIDE, SIDE, cap, part)
    result = pl.pallas_call(
        moe_kernel,
        out_shape=pltpu.VMEM((rows, part), F32),
        in_specs=[
            pl.BlockSpec(memory_space=pltpu.VMEM),
            pl.BlockSpec(memory_space=pltpu.VMEM),
            pl.BlockSpec(memory_space=pltpu.VMEM),
            pl.BlockSpec(memory_space=pl.ANY),
            pl.BlockSpec(memory_space=pltpu.VMEM),
            pl.BlockSpec(memory_space=pl.ANY),
            pl.BlockSpec(memory_space=pl.ANY),
            pl.BlockSpec(memory_space=pl.ANY),
        ],
        out_specs=pl.BlockSpec(memory_space=pltpu.VMEM),
        scratch_shapes=[
            vmem(rows, width),
            vmem(SIDE, rows, part),
            pltpu.VMEM((SIDE, 2, SIDE, 2 * rows), F32),
            pltpu.VMEM((SIDE, 2, SIDE, 2 * rows), F32),
            vmem(*blocks),
            vmem(*blocks),
            vmem(*blocks),
            vmem(2, part, hidden),
            vmem(2, part, hidden),
            vmem(2, hidden, part),
            pltpu.VMEM((SIDE, SIDE, cap, hidden), F32),
            pltpu.VMEM((SIDE, SIDE, cap, hidden), F32),
            vmem(SIDE, SIDE, cap, hidden),
            vmem(*blocks),
            vmem(*blocks),
            vmem(*blocks),
            vmem(*blocks),
            vmem(*blocks),
            vmem(SIDE, SUM_CUT, rows, part // SUM_CUT),
            vmem(SIDE, SUM_CUT, rows, part // SUM_CUT),
            pltpu.VMEM((2, rows, part), F32),
            dma((7,)),
            dma((SIDE, RING_CUT)),
            dma((SIDE, RING_CUT)),
            dma((SIDE, SUM_CUT)),
            dma((SIDE, SUM_CUT)),
        ]
        + [dma((SIDE,)) for _ in range(10)]
        + [pltpu.SemaphoreType.REGULAR],
        compiler_params=pltpu.CompilerParams(
            collective_id=0, has_side_effects=True, vmem_limit_bytes=60 * 1024 * 1024
        ),
        name="moe",
    )(
        route_ids.T, group_weight.T, expert_weight.T,
        tokens_in, norm_gain.reshape(1, width), gate_proj, up_proj, down_proj,
    )
    return result.astype(BF)


def solution(mesh):
    in_specs = (
        P(("grp", "ep"), None),
        P(),
        P("ep", None, "tp"),
        P("ep", None, "tp"),
        P("ep", "tp", None),
        P(("grp", "ep"), None),
        P(("grp", "ep"), None),
        P(("grp", "ep"), None),
    )
    out_specs = P(("grp", "ep"), "tp")
    return jax.shard_map(
        on_device, mesh=mesh, in_specs=in_specs, out_specs=out_specs, check_vma=False
    )
```

```python
import functools
import math

import jax
import jax.numpy as jnp
from jax import lax
from jax.experimental import pallas as pl
from jax.experimental.pallas import tpu as pltpu
from jax.sharding import PartitionSpec as P

TOP = 8
EXP_GRP = 8
EPSILON = 1e-06
MESH = pl.DeviceIdType.MESH
SIDE = 8
BF = jnp.bfloat16
F32 = jnp.float32

OFF = [0, 1, 7, 2, 6, 3, 5, 4]
BACK = [OFF.index((-o) % SIDE) for o in OFF]
FAR = SIDE - 1
INWARD_GROUPS = [(FAR,), (5, 6), (3, 4), (1, 2), (0,)]
INWARD = [s for places in INWARD_GROUPS for s in places]
RING_CUT = 4
SUM_CUT = 2
HELD_BACK = 5


def next_outward(place, p):
    if place + 2 < FAR:
        return place + 2
    return FAR if place == (6, 5)[p % 2] else None


def next_inward(place, p):
    if place == FAR:
        return ((5, 1), (6, 2))[p % 2]
    return {1: 0, 2: 6 + 1}.get(place, place - 2), 2 - place % 2


def sums_from(place, p):
    if place in (5, 6):
        return (place,) if place == (5, 6)[p % 2] else ()
    return {0: (0, 7), FAR: ()}.get(place, (place,))


def ring_offset(place):
    half = (place + 1) // 2
    odd = place % 2
    return (odd * half + (1 - odd) * (SIDE - half)) % SIDE


def moe_kernel(
    ids_ref, group_ref, weight_ref, tokens_hbm, gain_ref, gate_hbm, up_hbm, down_hbm, out_ref,
    tok_in, toks, meta_out, meta, sel, xin, xoth, wg, wu, wd, accg, accu, hid,
    part_out, part_own, part_in, res, ret, sums_out, sums_in, mixed,
    load_sem, ag_send, ag_recv, sum_send, sum_recv, meta_send, meta_recv, sel_send, xin_recv, xo_send, xo_recv,
    part_send, part_recv, res_send, ret_recv, lead_sem,
):
    rows, width = tok_in.shape
    part = width // 2
    cap = sel.shape[2]
    hidden = wg.shape[2]
    grp = lax.axis_index("grp")
    ep = lax.axis_index("ep")
    core = lax.axis_index("tp")
    up_y = ep // SIDE
    up_x = ep % SIDE
    first = up_x * (1 - core) + up_y * core
    second = up_y * (1 - core) + up_x * core
    step_first = (1 - core) + SIDE * core
    step_second = SIDE * (1 - core) + core

    def along_first(place):
        at = (first + OFF[place]) % SIDE
        return (grp, at * step_first + second * step_second, core)

    def along_second(place):
        at = (second + OFF[place]) % SIDE
        return (grp, first * step_first + at * step_second, core)

    partner = (grp, ep, 1 - core)

    peer_count = 2 * (SIDE - 1) + 1
    in_lead_row = (second == 0) & (core == 0)
    in_lead_column = (first == 0) & (core == 0)
    is_lead = in_lead_row & in_lead_column
    beside_lead = (ep == 0) & (core == 1)
    knows_lead = (in_lead_row | in_lead_column | beside_lead) & jnp.logical_not(is_lead)

    def signal_peers(semaphore):
        for place in range(1, SIDE):
            pl.semaphore_signal(semaphore, inc=1, device_id=along_first(place), device_id_type=MESH)
            pl.semaphore_signal(semaphore, inc=1, device_id=along_second(place), device_id_type=MESH)
        pl.semaphore_signal(semaphore, inc=1, device_id=partner, device_id_type=MESH)

    barrier = pltpu.get_barrier_semaphore()

    @pl.when(jnp.logical_not(is_lead))
    def _():
        signal_peers(barrier)

    @pl.when(is_lead)
    def _():
        pl.semaphore_wait(barrier, peer_count)
        signal_peers(lead_sem)

    def await_lead(who):
        @pl.when(who & jnp.logical_not(is_lead))
        def _():
            pl.semaphore_wait(lead_sem, 1)

    def send(src, dst, send_sem, recv_sem, to):
        copy = pltpu.make_async_remote_copy(
            src_ref=src, dst_ref=dst, send_sem=send_sem, recv_sem=recv_sem,
            device_id=to, device_id_type=MESH,
        )
        copy.start()

    def wait_bytes(ref, sem):
        pltpu.make_async_copy(ref, ref, sem).wait()

    own = pl.ds(pl.multiple_of(core * part, part), part)
    other = pl.ds(pl.multiple_of((1 - core) * part, part), part)
    tok_load = pltpu.make_async_copy(tokens_hbm, tok_in, load_sem.at[0])
    tok_load.start()
    loads = [
        pltpu.make_async_copy(gate_hbm.at[0, own], wg.at[0], load_sem.at[1]),
        pltpu.make_async_copy(up_hbm.at[0, own], wu.at[0], load_sem.at[2]),
        pltpu.make_async_copy(gate_hbm.at[0, other], wg.at[1], load_sem.at[3]),
        pltpu.make_async_copy(up_hbm.at[0, other], wu.at[1], load_sem.at[4]),
        pltpu.make_async_copy(down_hbm.at[0, :, own], wd.at[0], load_sem.at[5]),
        pltpu.make_async_copy(down_hbm.at[0, :, other], wd.at[1], load_sem.at[6]),
    ]
    for load in loads:
        load.start()

    tok_load.wait()
    values = tok_in[...].astype(F32)
    scale = lax.rsqrt(jnp.mean(values * values, axis=-1, keepdims=True) + EPSILON)
    toks[0] = (tok_in[:, own].astype(F32) * scale * gain_ref[:, own]).astype(BF)

    @pl.when(jnp.logical_not(is_lead))
    def _():
        pl.semaphore_wait(barrier, peer_count - knows_lead.astype(jnp.int32))

    def lead_at(up, follows):
        beyond = up // (SIDE // 2 + 1)
        place = (1 - beyond) * (2 * up - 1) + beyond * 2 * (SIDE - up)
        back = place + 2 * (place % 2) - 1 - place // FAR
        follows = (follows & jnp.logical_not(is_lead)).astype(jnp.int32)
        return place * follows - (1 - follows), back

    lead_slot, my_slot = lead_at((SIDE - first) % SIDE, in_lead_row)
    lead_place, my_place = lead_at((SIDE - second) % SIDE, in_lead_column)
    lead = (grp, 0, core)

    def piece(p):
        return pl.ds(p * (rows // RING_CUT), rows // RING_CUT)

    def pass_on(place, to_place, p):
        backward = place % 2 == 1 if place else to_place % 2 == 1
        send(
            toks.at[place, piece(p)], toks.at[to_place, piece(p)],
            ag_send.at[to_place, p], ag_recv.at[to_place, p], along_first(2 if backward else 1),
        )

    for p in range(RING_CUT):
        for place in (1, 2):
            pl.when(lead_slot != BACK[place])(functools.partial(pass_on, 0, place, p))

    lanes = 2 * rows
    experts = SIDE * SIDE
    row = lax.broadcasted_iota(jnp.int32, (experts, lanes), 0)
    lane = lax.broadcasted_iota(jnp.int32, (experts, lanes), 1)
    at_first = (first + ring_offset(row // SIDE)) % SIDE
    at_second = (second + ring_offset(row % SIDE)) % SIDE
    expert = at_first * step_first + at_second * step_second

    def across(ref):
        turned = ref[...].astype(F32)
        return jnp.concatenate([turned, turned], axis=1)

    ids, group_weights, weights = across(ids_ref), across(group_ref), across(weight_ref)
    weight_sum = jnp.sum(weights, axis=0, keepdims=True)
    named = jnp.zeros((experts, lanes), F32)
    weight = jnp.zeros((experts, lanes), F32)
    expert_f = expert.astype(F32)
    for k in range(TOP):
        match = expert_f == ids[k : k + 1, :]
        named = jnp.where(match, 1.0, named)
        weight = jnp.where(match, weights[k : k + 1, :], weight)
    group = expert // EXP_GRP
    group_part = jnp.zeros((experts, lanes), F32)
    for g in range(experts // EXP_GRP):
        group_part = jnp.where(group == g, group_weights[g : g + 1, :], group_part)
    gates = group_part * weight / weight_sum
    high = gates.astype(BF).astype(F32)
    gates = jnp.where(lane < rows, high, gates - high)
    before = lax.broadcasted_iota(jnp.int32, (lanes, lanes), 0)
    after = lax.broadcasted_iota(jnp.int32, (lanes, lanes), 1)
    earlier = jnp.where((before < after) & (before // rows == after // rows), 1.0, 0.0).astype(BF)
    rank = jnp.dot(named.astype(BF), earlier, preferred_element_type=F32)
    slots = jnp.where(named > 0.0, rank, -1.0)
    meta_out[:, 0] = slots.reshape(SIDE, SIDE, lanes)
    meta_out[:, 1] = gates.reshape(SIDE, SIDE, lanes)
    meta[0] = meta_out[0]

    def send_meta(place, slot, to):
        send(meta_out.at[place], meta.at[slot], meta_send.at[place], meta_recv.at[slot], to)

    for place in range(1, SIDE):
        pl.when(lead_slot != place)(functools.partial(send_meta, place, BACK[place], along_first(place)))
    accg[...] = jnp.zeros_like(accg)
    accu[...] = jnp.zeros_like(accu)

    slot_iota = (lax.broadcasted_iota(jnp.int32, (SIDE * cap, lanes), 0) % cap).astype(F32)

    def spread(table):
        return jnp.concatenate(
            [jnp.broadcast_to(table[j : j + 1, :], (cap, lanes)) for j in range(SIDE)], axis=0
        )

    def receive(places):
        for p in range(RING_CUT):
            for s in places:
                if s > 0:
                    wait_bytes(toks.at[s, piece(p)], ag_recv.at[s, p])
                    onward = next_outward(s, p)
                    if onward:
                        pass_on(s, onward, p)

    def pick_and_send(s):
        if s > 0:
            wait_bytes(meta.at[s], meta_recv.at[s])
        chosen = jnp.where(spread(meta[s, 0]) == slot_iota, 1.0, 0.0).astype(BF)[:, :rows]
        picked = jnp.dot(chosen, toks[s], preferred_element_type=F32).astype(BF)
        picked = picked.reshape(SIDE, cap, part)
        sel[s] = picked
        xin[s, 0] = picked[0]
        for place in range(SIDE - 1, 0, -1):

            def send_rows():
                send(sel.at[s, place], xin.at[s, BACK[place]], sel_send.at[s], xin_recv.at[s], along_second(place))

            if s < HELD_BACK:
                pl.when(place != lead_place)(send_rows)
            else:
                send_rows()

    def multiply_in(block, at, half):
        for acc, weights in ((accg, wg), (accu, wu)):
            acts = jnp.dot(block.reshape(-1, part), weights[half], preferred_element_type=F32)
            acc[at] += acts.reshape(block.shape[:-1] + (hidden,))

    def take_own(s, count=1):
        for one in range(s, s + count):
            wait_bytes(xin.at[one, pl.ds(1, SIDE - 1)], xin_recv.at[one])
            send(xin.at[one], xoth.at[:, one], xo_send.at[one], xo_recv.at[one], partner)
        multiply_in(xin[s : s + count], (pl.ds(s, count),), 0)

    def take_other(s, count=1):
        for one in range(s, s + count):
            wait_bytes(xoth.at[:, one], xo_recv.at[one])
        multiply_in(xoth[:, s : s + count], (slice(None), pl.ds(s, count)), 1)

    def activate(*at):
        gate_acts = accg[at]
        hid[at] = (gate_acts / (1.0 + jnp.exp(-gate_acts)) * accu[at]).astype(BF)

    early = in_lead_row & jnp.logical_not(is_lead)

    def when(condition, *work):
        @pl.when(condition)
        def _():
            for take, s in work:
                take(s, 2)

    def greet_lead(near):
        known = in_lead_row & jnp.logical_not(is_lead)
        mine = known & ((lead_slot < 3) if near else (lead_slot > 2))
        await_lead(mine)

        @pl.when(mine)
        def _():
            send_meta(lead_slot, my_slot, lead)

        if near:
            for place in (1, 2):

                @pl.when(lead_slot == BACK[place])
                def _():
                    for p in range(RING_CUT):
                        pass_on(0, place, p)

    greet_lead(True)
    receive((1, 2))
    greet_lead(False)
    for s in (0, 1, 2):
        pick_and_send(s)
    receive((3, 4))
    for s in (3, 4):
        pick_and_send(s)
    await_lead(in_lead_column)

    @pl.when(lead_place > 0)
    def _():
        for s in range(HELD_BACK):
            send(sel.at[s, lead_place], xin.at[s, my_place], sel_send.at[s], xin_recv.at[s], lead)

    for load in loads:
        load.wait()
    when(early, (take_own, 0))
    receive((5, 6))
    for s in (5, 6):
        pick_and_send(s)
    when(early, (take_own, 2), (take_other, 0))
    when(is_lead, (take_own, 0))
    receive((FAR,))
    pick_and_send(FAR)
    await_lead(beside_lead)
    when(jnp.logical_not(in_lead_row), (take_own, 0))
    when(jnp.logical_not(early), (take_own, 2), (take_other, 0))
    take_own(4, 2)
    take_other(2, 2)
    take_own(FAR - 1)
    take_other(4, 2)
    take_other(FAR - 1)
    take_own(FAR)
    for s in range(FAR):
        activate(s, pl.ds(0, FAR))
    take_other(FAR)
    activate(FAR)
    activate(pl.ds(0, FAR), FAR)

    def multiply_down(s):
        theirs = hid[:, s].reshape(SIDE * cap, hidden)
        part_out[s] = jnp.dot(theirs, wd[1], preferred_element_type=F32).astype(BF).reshape(SIDE, cap, part)
        send(part_out.at[s], part_in.at[s], part_send.at[s], part_recv.at[s], partner)
        mine = hid[s].reshape(SIDE * cap, hidden)
        part_own[s] = jnp.dot(mine, wd[0], preferred_element_type=F32).astype(BF).reshape(SIDE, cap, part)

    def return_rows(s):
        wait_bytes(part_in.at[s], part_recv.at[s])
        res[s] = (part_own[s].astype(F32) + part_in[s].astype(F32)).astype(BF)
        ret[s, 0] = res[s, 0]
        for place in range(SIDE - 1, 0, -1):
            send(res.at[s, place], ret.at[s, BACK[place]], res_send.at[s], ret_recv.at[s], along_second(place))

    columns = part // SUM_CUT

    def mix(s, at):
        wait_bytes(ret.at[s, pl.ds(1, SIDE - 1)], ret_recv.at[s])
        mixer = jnp.where(spread(meta[s, 0]) == slot_iota, spread(meta[s, 1]), 0.0).astype(BF)
        both = lax.dot_general(
            mixer, ret[s].reshape(SIDE * cap, part), (((0,), (0,)), ((), ())), preferred_element_type=F32
        )
        mixed[at] = both[:rows] + both[rows:]

    def pass_sum(s, at, p):
        total = mixed[at, :, p * columns : (p + 1) * columns]
        for slot in sums_from(s, p):
            wait_bytes(sums_in.at[slot, p], sum_recv.at[slot, p])
            total = total + sums_in[slot, p].astype(F32)
        if s == 0:
            out_ref[:, p * columns : (p + 1) * columns] = total
            return
        sums_out[s, p] = total.astype(BF)
        to_slot, toward = next_inward(s, p)
        send(
            sums_out.at[s, p], sums_in.at[to_slot, p], sum_send.at[s, p], sum_recv.at[to_slot, p], along_first(toward)
        )

    for step in range(SIDE + 1):
        if step < SIDE:
            multiply_down(INWARD[step])
        if 1 <= step:
            return_rows(INWARD[step - 1])
    for places in INWARD_GROUPS:
        for at, s in enumerate(places):
            mix(s, at)
        for p in range(SUM_CUT):
            for at, s in enumerate(places):
                pass_sum(s, at, p)

    for place in range(1, SIDE):
        wait_bytes(meta_out.at[place], meta_send.at[place])
        for p in range(RING_CUT):
            wait_bytes(toks.at[place, piece(p)], ag_send.at[place, p])
        for p in range(SUM_CUT):
            wait_bytes(sums_out.at[place, p], sum_send.at[place, p])
    for s in range(SIDE):
        wait_bytes(sel.at[s, pl.ds(1, SIDE - 1)], sel_send.at[s])
        wait_bytes(xin.at[s], xo_send.at[s])
        wait_bytes(part_out.at[s], part_send.at[s])
        wait_bytes(res.at[s, pl.ds(1, SIDE - 1)], res_send.at[s])


def on_device(
    tokens_in, norm_gain, gate_proj, up_proj, down_proj, route_ids, group_weight, expert_weight
):
    rows, width = tokens_in.shape
    experts = gate_proj.shape[0] * lax.axis_size("ep")
    hidden = gate_proj.shape[2]
    cap = min(rows, max(2, 2 * rows * TOP // experts))
    part = width // 2
    vmem = lambda *shape: pltpu.VMEM(shape, BF)
    dma = pltpu.SemaphoreType.DMA
    blocks = (SIDE, SIDE, cap, part)
    result = pl.pallas_call(
        moe_kernel,
        out_shape=pltpu.VMEM((rows, part), F32),
        in_specs=[
            pl.BlockSpec(memory_space=pltpu.VMEM),
            pl.BlockSpec(memory_space=pltpu.VMEM),
            pl.BlockSpec(memory_space=pltpu.VMEM),
            pl.BlockSpec(memory_space=pl.ANY),
            pl.BlockSpec(memory_space=pltpu.VMEM),
            pl.BlockSpec(memory_space=pl.ANY),
            pl.BlockSpec(memory_space=pl.ANY),
            pl.BlockSpec(memory_space=pl.ANY),
        ],
        out_specs=pl.BlockSpec(memory_space=pltpu.VMEM),
        scratch_shapes=[
            vmem(rows, width),
            vmem(SIDE, rows, part),
            pltpu.VMEM((SIDE, 2, SIDE, 2 * rows), F32),
            pltpu.VMEM((SIDE, 2, SIDE, 2 * rows), F32),
            vmem(*blocks),
            vmem(*blocks),
            vmem(*blocks),
            vmem(2, part, hidden),
            vmem(2, part, hidden),
            vmem(2, hidden, part),
            pltpu.VMEM((SIDE, SIDE, cap, hidden), F32),
            pltpu.VMEM((SIDE, SIDE, cap, hidden), F32),
            vmem(SIDE, SIDE, cap, hidden),
            vmem(*blocks),
            vmem(*blocks),
            vmem(*blocks),
            vmem(*blocks),
            vmem(*blocks),
            vmem(SIDE, SUM_CUT, rows, part // SUM_CUT),
            vmem(SIDE, SUM_CUT, rows, part // SUM_CUT),
            pltpu.VMEM((2, rows, part), F32),
            dma((7,)),
            dma((SIDE, RING_CUT)),
            dma((SIDE, RING_CUT)),
            dma((SIDE, SUM_CUT)),
            dma((SIDE, SUM_CUT)),
        ]
        + [dma((SIDE,)) for _ in range(10)]
        + [pltpu.SemaphoreType.REGULAR],
        compiler_params=pltpu.CompilerParams(
            collective_id=0, has_side_effects=True, vmem_limit_bytes=60 * 1024 * 1024
        ),
        name="moe",
    )(
        route_ids.T, group_weight.T, expert_weight.T,
        tokens_in, norm_gain.reshape(1, width), gate_proj, up_proj, down_proj,
    )
    return result.astype(BF)


def solution(mesh):
    in_specs = (
        P(("grp", "ep"), None),
        P(),
        P("ep", None, "tp"),
        P("ep", None, "tp"),
        P("ep", "tp", None),
        P(("grp", "ep"), None),
        P(("grp", "ep"), None),
        P(("grp", "ep"), None),
    )
    out_specs = P(("grp", "ep"), "tp")
    return jax.shard_map(
        on_device, mesh=mesh, in_specs=in_specs, out_specs=out_specs, check_vma=False
    )
```

```python
import functools
import math

import jax
import jax.numpy as jnp
from jax import lax
from jax.experimental import pallas as pl
from jax.experimental.pallas import tpu as pltpu
from jax.sharding import PartitionSpec as P

TOP = 8
EXP_GRP = 8
EPSILON = 1e-06
MESH = pl.DeviceIdType.MESH
SIDE = 8
BF = jnp.bfloat16
F32 = jnp.float32

OFF = [0, 1, 7, 2, 6, 3, 5, 4]
BACK = [OFF.index((-o) % SIDE) for o in OFF]
FAR = SIDE - 1
INWARD_GROUPS = [(FAR,), (5, 6), (3, 4), (1, 2), (0,)]
INWARD = [s for places in INWARD_GROUPS for s in places]
RING_CUT = 8
SUM_CUT = 2
HELD_BACK = 5


def next_outward(place, p):
    if place + 2 < FAR:
        return place + 2
    return FAR if place == (6, 5)[p % 2] else None


def next_inward(place, p):
    if place == FAR:
        return ((5, 1), (6, 2))[p % 2]
    return {1: 0, 2: 6 + 1}.get(place, place - 2), 2 - place % 2


def sums_from(place, p):
    if place in (5, 6):
        return (place,) if place == (5, 6)[p % 2] else ()
    return {0: (0, 7), FAR: ()}.get(place, (place,))


def ring_offset(place):
    half = (place + 1) // 2
    odd = place % 2
    return (odd * half + (1 - odd) * (SIDE - half)) % SIDE


def moe_kernel(
    ids_ref, group_ref, weight_ref, tokens_hbm, gain_ref, gate_hbm, up_hbm, down_hbm, out_ref,
    tok_in, toks, meta_out, meta, sel, xin, xoth, wg, wu, wd, accg, accu, hid,
    part_out, part_own, part_in, res, ret, sums_out, sums_in, mixed,
    load_sem, ag_send, ag_recv, sum_send, sum_recv, meta_send, meta_recv, sel_send, xin_recv, xo_send, xo_recv,
    part_send, part_recv, res_send, ret_recv, lead_sem,
):
    rows, width = tok_in.shape
    part = width // 2
    cap = sel.shape[2]
    hidden = wg.shape[2]
    grp = lax.axis_index("grp")
    ep = lax.axis_index("ep")
    core = lax.axis_index("tp")
    up_y = ep // SIDE
    up_x = ep % SIDE
    first = up_x * (1 - core) + up_y * core
    second = up_y * (1 - core) + up_x * core
    step_first = (1 - core) + SIDE * core
    step_second = SIDE * (1 - core) + core

    def along_first(place):
        at = (first + OFF[place]) % SIDE
        return (grp, at * step_first + second * step_second, core)

    def along_second(place):
        at = (second + OFF[place]) % SIDE
        return (grp, first * step_first + at * step_second, core)

    partner = (grp, ep, 1 - core)

    peer_count = 2 * (SIDE - 1) + 1
    in_lead_row = (second == 0) & (core == 0)
    in_lead_column = (first == 0) & (core == 0)
    is_lead = in_lead_row & in_lead_column
    beside_lead = (ep == 0) & (core == 1)
    knows_lead = (in_lead_row | in_lead_column | beside_lead) & jnp.logical_not(is_lead)

    def signal_peers(semaphore):
        for place in range(1, SIDE):
            pl.semaphore_signal(semaphore, inc=1, device_id=along_first(place), device_id_type=MESH)
            pl.semaphore_signal(semaphore, inc=1, device_id=along_second(place), device_id_type=MESH)
        pl.semaphore_signal(semaphore, inc=1, device_id=partner, device_id_type=MESH)

    barrier = pltpu.get_barrier_semaphore()

    @pl.when(jnp.logical_not(is_lead))
    def _():
        signal_peers(barrier)

    def await_lead(who):
        @pl.when(who & jnp.logical_not(is_lead))
        def _():
            pl.semaphore_wait(lead_sem, 1)

    def send(src, dst, send_sem, recv_sem, to):
        copy = pltpu.make_async_remote_copy(
            src_ref=src, dst_ref=dst, send_sem=send_sem, recv_sem=recv_sem,
            device_id=to, device_id_type=MESH,
        )
        copy.start()

    def wait_bytes(ref, sem):
        pltpu.make_async_copy(ref, ref, sem).wait()

    own = pl.ds(pl.multiple_of(core * part, part), part)
    other = pl.ds(pl.multiple_of((1 - core) * part, part), part)
    tok_load = pltpu.make_async_copy(tokens_hbm, tok_in, load_sem.at[0])
    tok_load.start()
    loads = [
        pltpu.make_async_copy(gate_hbm.at[0, own], wg.at[0], load_sem.at[1]),
        pltpu.make_async_copy(up_hbm.at[0, own], wu.at[0], load_sem.at[2]),
        pltpu.make_async_copy(gate_hbm.at[0, other], wg.at[1], load_sem.at[3]),
        pltpu.make_async_copy(up_hbm.at[0, other], wu.at[1], load_sem.at[4]),
        pltpu.make_async_copy(down_hbm.at[0, :, own], wd.at[0], load_sem.at[5]),
        pltpu.make_async_copy(down_hbm.at[0, :, other], wd.at[1], load_sem.at[6]),
    ]
    for load in loads:
        load.start()

    tok_load.wait()
    values = tok_in[...].astype(F32)
    scale = lax.rsqrt(jnp.mean(values * values, axis=-1, keepdims=True) + EPSILON)
    toks[0] = (tok_in[:, own].astype(F32) * scale * gain_ref[:, own]).astype(BF)

    pl.semaphore_wait(barrier, peer_count - knows_lead.astype(jnp.int32))

    @pl.when(is_lead)
    def _():
        signal_peers(lead_sem)

    await_lead(in_lead_row)

    def piece(p):
        return pl.ds(p * (rows // RING_CUT), rows // RING_CUT)

    def pass_on(place, to_place, p):
        backward = place % 2 == 1 if place else to_place % 2 == 1
        send(
            toks.at[place, piece(p)], toks.at[to_place, piece(p)],
            ag_send.at[to_place, p], ag_recv.at[to_place, p], along_first(2 if backward else 1),
        )

    for p in range(RING_CUT):
        pass_on(0, 1, p)
        pass_on(0, 2, p)

    lanes = 2 * rows
    experts = SIDE * SIDE
    row = lax.broadcasted_iota(jnp.int32, (experts, lanes), 0)
    lane = lax.broadcasted_iota(jnp.int32, (experts, lanes), 1)
    at_first = (first + ring_offset(row // SIDE)) % SIDE
    at_second = (second + ring_offset(row % SIDE)) % SIDE
    expert = at_first * step_first + at_second * step_second

    def across(ref):
        turned = ref[...].astype(F32)
        return jnp.concatenate([turned, turned], axis=1)

    ids, group_weights, weights = across(ids_ref), across(group_ref), across(weight_ref)
    weight_sum = jnp.sum(weights, axis=0, keepdims=True)
    named = jnp.zeros((experts, lanes), F32)
    weight = jnp.zeros((experts, lanes), F32)
    expert_f = expert.astype(F32)
    for k in range(TOP):
        match = expert_f == ids[k : k + 1, :]
        named = jnp.where(match, 1.0, named)
        weight = jnp.where(match, weights[k : k + 1, :], weight)
    group = expert // EXP_GRP
    group_part = jnp.zeros((experts, lanes), F32)
    for g in range(experts // EXP_GRP):
        group_part = jnp.where(group == g, group_weights[g : g + 1, :], group_part)
    gates = group_part * weight / weight_sum
    high = gates.astype(BF).astype(F32)
    gates = jnp.where(lane < rows, high, gates - high)
    before = lax.broadcasted_iota(jnp.int32, (lanes, lanes), 0)
    after = lax.broadcasted_iota(jnp.int32, (lanes, lanes), 1)
    earlier = jnp.where((before < after) & (before // rows == after // rows), 1.0, 0.0).astype(BF)
    rank = jnp.dot(named.astype(BF), earlier, preferred_element_type=F32)
    slots = jnp.where(named > 0.0, rank, -1.0)
    meta_out[:, 0] = slots.reshape(SIDE, SIDE, lanes)
    meta_out[:, 1] = gates.reshape(SIDE, SIDE, lanes)
    meta[0] = meta_out[0]

    for place in range(1, SIDE):
        send(meta_out.at[place], meta.at[BACK[place]], meta_send.at[place], meta_recv.at[BACK[place]], along_first(place))
    accg[...] = jnp.zeros_like(accg)
    accu[...] = jnp.zeros_like(accu)

    slot_iota = (lax.broadcasted_iota(jnp.int32, (SIDE * cap, lanes), 0) % cap).astype(F32)

    def spread(table):
        return jnp.concatenate(
            [jnp.broadcast_to(table[j : j + 1, :], (cap, lanes)) for j in range(SIDE)], axis=0
        )

    def receive(places):
        for p in range(RING_CUT):
            for s in places:
                if s > 0:
                    wait_bytes(toks.at[s, piece(p)], ag_recv.at[s, p])
                    onward = next_outward(s, p)
                    if onward:
                        pass_on(s, onward, p)

    up = (SIDE - second) % SIDE
    beyond = up // (SIDE // 2 + 1)
    lead_place = (1 - beyond) * (2 * up - 1) + beyond * 2 * (SIDE - up)
    my_place = lead_place + 2 * (lead_place % 2) - 1 - lead_place // FAR
    follows = (in_lead_column & jnp.logical_not(is_lead)).astype(jnp.int32)
    lead_place = lead_place * follows - (1 - follows)
    lead = (grp, 0, core)

    def pick_and_send(s):
        if s > 0:
            wait_bytes(meta.at[s], meta_recv.at[s])
        chosen = jnp.where(spread(meta[s, 0]) == slot_iota, 1.0, 0.0).astype(BF)[:, :rows]
        picked = jnp.dot(chosen, toks[s], preferred_element_type=F32).astype(BF)
        picked = picked.reshape(SIDE, cap, part)
        sel[s] = picked
        xin[s, 0] = picked[0]
        for place in range(SIDE - 1, 0, -1):

            def send_rows():
                send(sel.at[s, place], xin.at[s, BACK[place]], sel_send.at[s], xin_recv.at[s], along_second(place))

            if s < HELD_BACK:
                pl.when(place != lead_place)(send_rows)
            else:
                send_rows()

    def multiply_in(block, at, half):
        for acc, weights in ((accg, wg), (accu, wu)):
            acts = jnp.dot(block.reshape(-1, part), weights[half], preferred_element_type=F32)
            acc[at] += acts.reshape(block.shape[:-1] + (hidden,))

    def take_own(s, count=1):
        for one in range(s, s + count):
            wait_bytes(xin.at[one, pl.ds(1, SIDE - 1)], xin_recv.at[one])
            send(xin.at[one], xoth.at[:, one], xo_send.at[one], xo_recv.at[one], partner)
        multiply_in(xin[s : s + count], (pl.ds(s, count),), 0)

    def take_other(s, count=1):
        for one in range(s, s + count):
            wait_bytes(xoth.at[:, one], xo_recv.at[one])
        multiply_in(xoth[:, s : s + count], (slice(None), pl.ds(s, count)), 1)

    def activate(*at):
        gate_acts = accg[at]
        hid[at] = (gate_acts / (1.0 + jnp.exp(-gate_acts)) * accu[at]).astype(BF)

    early = in_lead_row & jnp.logical_not(is_lead)

    def when(condition, *work):
        @pl.when(condition)
        def _():
            for take, s in work:
                take(s, 2)

    receive((1, 2))
    for s in (0, 1, 2):
        pick_and_send(s)
    receive((3, 4))
    for s in (3, 4):
        pick_and_send(s)
    await_lead(in_lead_column)

    @pl.when(lead_place > 0)
    def _():
        for s in range(HELD_BACK):
            send(sel.at[s, lead_place], xin.at[s, my_place], sel_send.at[s], xin_recv.at[s], lead)

    for load in loads:
        load.wait()
    when(early, (take_own, 0))
    receive((5, 6))
    for s in (5, 6):
        pick_and_send(s)
    when(early, (take_own, 2), (take_other, 0))
    when(is_lead, (take_own, 0))
    receive((FAR,))
    pick_and_send(FAR)
    await_lead(beside_lead)
    when(jnp.logical_not(in_lead_row), (take_own, 0))
    when(jnp.logical_not(early), (take_own, 2), (take_other, 0))
    take_own(4, 2)
    take_other(2, 2)
    take_own(FAR - 1)
    take_other(4, 2)
    take_other(FAR - 1)
    take_own(FAR)
    for s in range(FAR):
        activate(s, pl.ds(0, FAR))
    take_other(FAR)
    activate(FAR)
    activate(pl.ds(0, FAR), FAR)

    def multiply_down(s):
        theirs = hid[:, s].reshape(SIDE * cap, hidden)
        part_out[s] = jnp.dot(theirs, wd[1], preferred_element_type=F32).astype(BF).reshape(SIDE, cap, part)
        send(part_out.at[s], part_in.at[s], part_send.at[s], part_recv.at[s], partner)
        mine = hid[s].reshape(SIDE * cap, hidden)
        part_own[s] = jnp.dot(mine, wd[0], preferred_element_type=F32).astype(BF).reshape(SIDE, cap, part)

    def return_rows(s):
        wait_bytes(part_in.at[s], part_recv.at[s])
        res[s] = (part_own[s].astype(F32) + part_in[s].astype(F32)).astype(BF)
        ret[s, 0] = res[s, 0]
        for place in range(SIDE - 1, 0, -1):
            send(res.at[s, place], ret.at[s, BACK[place]], res_send.at[s], ret_recv.at[s], along_second(place))

    columns = part // SUM_CUT

    def mix(s, at):
        wait_bytes(ret.at[s, pl.ds(1, SIDE - 1)], ret_recv.at[s])
        mixer = jnp.where(spread(meta[s, 0]) == slot_iota, spread(meta[s, 1]), 0.0).astype(BF)
        both = lax.dot_general(
            mixer, ret[s].reshape(SIDE * cap, part), (((0,), (0,)), ((), ())), preferred_element_type=F32
        )
        mixed[at] = both[:rows] + both[rows:]

    def pass_sum(s, at, p):
        total = mixed[at, :, p * columns : (p + 1) * columns]
        for slot in sums_from(s, p):
            wait_bytes(sums_in.at[slot, p], sum_recv.at[slot, p])
            total = total + sums_in[slot, p].astype(F32)
        if s == 0:
            out_ref[:, p * columns : (p + 1) * columns] = total
            return
        sums_out[s, p] = total.astype(BF)
        to_slot, toward = next_inward(s, p)
        send(
            sums_out.at[s, p], sums_in.at[to_slot, p], sum_send.at[s, p], sum_recv.at[to_slot, p], along_first(toward)
        )

    for step in range(SIDE + 1):
        if step < SIDE:
            multiply_down(INWARD[step])
        if 1 <= step:
            return_rows(INWARD[step - 1])
    for places in INWARD_GROUPS:
        for at, s in enumerate(places):
            mix(s, at)
        for p in range(SUM_CUT):
            for at, s in enumerate(places):
                pass_sum(s, at, p)

    for place in range(1, SIDE):
        wait_bytes(meta_out.at[place], meta_send.at[place])
        for p in range(RING_CUT):
            wait_bytes(toks.at[place, piece(p)], ag_send.at[place, p])
        for p in range(SUM_CUT):
            wait_bytes(sums_out.at[place, p], sum_send.at[place, p])
    for s in range(SIDE):
        wait_bytes(sel.at[s, pl.ds(1, SIDE - 1)], sel_send.at[s])
        wait_bytes(xin.at[s], xo_send.at[s])
        wait_bytes(part_out.at[s], part_send.at[s])
        wait_bytes(res.at[s, pl.ds(1, SIDE - 1)], res_send.at[s])


def on_device(
    tokens_in, norm_gain, gate_proj, up_proj, down_proj, route_ids, group_weight, expert_weight
):
    rows, width = tokens_in.shape
    experts = gate_proj.shape[0] * lax.axis_size("ep")
    hidden = gate_proj.shape[2]
    cap = min(rows, max(2, 2 * rows * TOP // experts))
    part = width // 2
    vmem = lambda *shape: pltpu.VMEM(shape, BF)
    dma = pltpu.SemaphoreType.DMA
    blocks = (SIDE, SIDE, cap, part)
    result = pl.pallas_call(
        moe_kernel,
        out_shape=pltpu.VMEM((rows, part), F32),
        in_specs=[
            pl.BlockSpec(memory_space=pltpu.VMEM),
            pl.BlockSpec(memory_space=pltpu.VMEM),
            pl.BlockSpec(memory_space=pltpu.VMEM),
            pl.BlockSpec(memory_space=pl.ANY),
            pl.BlockSpec(memory_space=pltpu.VMEM),
            pl.BlockSpec(memory_space=pl.ANY),
            pl.BlockSpec(memory_space=pl.ANY),
            pl.BlockSpec(memory_space=pl.ANY),
        ],
        out_specs=pl.BlockSpec(memory_space=pltpu.VMEM),
        scratch_shapes=[
            vmem(rows, width),
            vmem(SIDE, rows, part),
            pltpu.VMEM((SIDE, 2, SIDE, 2 * rows), F32),
            pltpu.VMEM((SIDE, 2, SIDE, 2 * rows), F32),
            vmem(*blocks),
            vmem(*blocks),
            vmem(*blocks),
            vmem(2, part, hidden),
            vmem(2, part, hidden),
            vmem(2, hidden, part),
            pltpu.VMEM((SIDE, SIDE, cap, hidden), F32),
            pltpu.VMEM((SIDE, SIDE, cap, hidden), F32),
            vmem(SIDE, SIDE, cap, hidden),
            vmem(*blocks),
            vmem(*blocks),
            vmem(*blocks),
            vmem(*blocks),
            vmem(*blocks),
            vmem(SIDE, SUM_CUT, rows, part // SUM_CUT),
            vmem(SIDE, SUM_CUT, rows, part // SUM_CUT),
            pltpu.VMEM((2, rows, part), F32),
            dma((7,)),
            dma((SIDE, RING_CUT)),
            dma((SIDE, RING_CUT)),
            dma((SIDE, SUM_CUT)),
            dma((SIDE, SUM_CUT)),
        ]
        + [dma((SIDE,)) for _ in range(10)]
        + [pltpu.SemaphoreType.REGULAR],
        compiler_params=pltpu.CompilerParams(
            collective_id=0, has_side_effects=True, vmem_limit_bytes=60 * 1024 * 1024
        ),
        name="moe",
    )(
        route_ids.T, group_weight.T, expert_weight.T,
        tokens_in, norm_gain.reshape(1, width), gate_proj, up_proj, down_proj,
    )
    return result.astype(BF)


def solution(mesh):
    in_specs = (
        P(("grp", "ep"), None),
        P(),
        P("ep", None, "tp"),
        P("ep", None, "tp"),
        P("ep", "tp", None),
        P(("grp", "ep"), None),
        P(("grp", "ep"), None),
        P(("grp", "ep"), None),
    )
    out_specs = P(("grp", "ep"), "tp")
    return jax.shard_map(
        on_device, mesh=mesh, in_specs=in_specs, out_specs=out_specs, check_vma=False
    )
```
